32 devices in a mesh: sp: 8 (over z, y), dp: 4 (over x, core).
Axes of the slice: x: 2, y: 2, z: 4, core: 2. Of those that a mesh axis runs over, the one named last changes fastest.
Arguments:
- residual: bfloat16 [4, 1024, 2048], P('dp', 'sp'), may hold values from -6 to 6
- query: bfloat16 [4, 1024, 1536], P('dp', 'sp'), may hold values from -64 to 64
- latent: bfloat16 [4, 1024, 256], P('dp', 'sp'), may hold values from -6 to 6
- rope_key: bfloat16 [4, 1024, 32], P('dp', 'sp'), may hold values from -64 to 64
- latent_gain: float32 [256], replicated, may hold values from 0.1 to 1.9
- query_gain: float32 [96], replicated, may hold values from 0.7 to 5.6
- key_gain: float32 [96], replicated, may hold values from 0.7 to 5.6
- key_weight: bfloat16 [256, 1024], replicated, may hold values from -0.375 to 0.375
- value_weight: bfloat16 [256, 1024], replicated, may hold values from -0.375 to 0.375
- mix_gain: float32 [1024], replicated, may hold values from 0.1 to 1.9
- out_weight: bfloat16 [1024, 2048], replicated, may hold values from -0.1875 to 0.1875
- ffn_gain: float32 [2048], replicated, may hold values from 0.1 to 1.9
- expert_choice: int32 [4, 1024, 2], P('dp', 'sp'), may hold values from 0 to 31, as said below
- group_prob: float32 [4, 1024], P('dp', 'sp'), may hold values from 0.25 to 1
- expert_prob: float32 [4, 1024, 2], P('dp', 'sp'), may hold values from 0.05 to 1
- gate_weight: bfloat16 [32, 2048, 512], P(('sp', 'dp')), may hold values from -0.125 to 0.125
- up_weight: bfloat16 [32, 2048, 512], P(('sp', 'dp')), may hold values from -0.125 to 0.125
- down_weight: bfloat16 [32, 512, 2048], P(('sp', 'dp')), may hold values from -0.25 to 0.25
Outputs:
- layer_out: bfloat16 [4, 1024, 2048], P('dp', 'sp')
The draws below stay inside these ranges and needn't reach their ends.
Inputs may be any that keep to these rules, and one draw needn't show every extreme that they name: `expert_choice`: A token's two experts differ and lie in one group of 8 consecutive expert numbers. In each aligned block of 128 tokens (the tokens of one device) no expert is named more than 16 times, and every expert of one group is named exactly 16 times in every block.
All inputs are finite; a program needn't handle non-finite values.
Results may differ from the reference program's by a relative error of at most 0.012.
The reference program's roundings to bfloat16 on the way count: a program that leaves them out, or rounds other values in their place, can miss the bound.
Values may be sent and summed in bfloat16 or wider, within the bound.
A program may use at most 64 MiB of HBM per device.

```python
import jax
import jax.numpy as jnp
from jax import lax

D = 2048
HEADS = 16
NOPE = 64
ROPE = 32
VDIM = 64
LATENT = 256
FF = 512
GROUPS = 4
TOP = 2
SPAN = 64
TOK_DEV = 128
QK = 96
LENGTH = 1024
BATCH = 4
EXPERTS = 32
EPG = 8
CAP = 16
N_SP = 8
N_DP = 4


def paired_rows(key):
    base_key = jax.random.fold_in(key, 11)
    query_key, rope_draw_key = jax.random.split(base_key, 2)
    query_all = jax.random.truncated_normal(query_key, -4.0, 4.0, (BATCH, LENGTH, HEADS, QK), jnp.float32)
    rope_all = jax.random.truncated_normal(rope_draw_key, -4.0, 4.0, (BATCH, LENGTH, ROPE), jnp.float32)
    return (query_all.reshape(BATCH, LENGTH, HEADS * QK), rope_all)


def draw_query(key, part):
    return paired_rows(key)[0].astype(jnp.bfloat16)


def draw_rope_key(key, part):
    return paired_rows(key)[1].astype(jnp.bfloat16)


def head_gains(key, salt):
    gain_key = jax.random.fold_in(key, salt)
    gains = jax.random.uniform(gain_key, (QK,), jnp.float32, 0.7, 1.3)
    return gains


def draw_query_gain(key, part):
    return head_gains(key, 21)


def draw_key_gain(key, part):
    return head_gains(key, 22)


def draw_expert_choice(key, part):
    base_key = jax.random.fold_in(key, 31)
    hot_key, block_key = jax.random.split(base_key)
    half_rows = TOK_DEV // 2
    block_total = BATCH * LENGTH // TOK_DEV
    hot_group = jax.random.randint(hot_key, (), 0, GROUPS)

    def one_block(sub_key):
        cut_key, offset_key, shift_key, order_key = jax.random.split(sub_key, 4)
        cuts = jnp.sort(jax.random.randint(cut_key, (2,), 0, half_rows + 1))
        position = jnp.arange(TOK_DEV, dtype=jnp.int32)
        rest_pos = position - half_rows
        other_index = (rest_pos >= cuts[0]).astype(jnp.int32) + (rest_pos >= cuts[1]).astype(jnp.int32)
        other_group = (hot_group + 1 + other_index) % GROUPS
        group_of = jnp.where(position < half_rows, hot_group, other_group)
        other_start = jnp.where(other_index == 0, half_rows, jnp.where(other_index == 1, half_rows + cuts[0], half_rows + cuts[1]))
        group_start = jnp.where(position < half_rows, 0, other_start)
        rank_in = position - group_start
        offsets = jax.random.randint(offset_key, (GROUPS,), 0, EPG)
        shifts = jax.random.randint(shift_key, (GROUPS,), 1, EPG)
        first_local = (rank_in + offsets[group_of]) % EPG
        second_local = (first_local + shifts[group_of]) % EPG
        pairs = jnp.stack([group_of * EPG + first_local, group_of * EPG + second_local], axis=-1)
        shuffle = jax.random.permutation(order_key, TOK_DEV)
        return pairs[shuffle]
    blocks = jax.vmap(one_block)(jax.random.split(block_key, block_total))
    return blocks.reshape(BATCH, LENGTH, TOP).astype(jnp.int32)


def shard_levels(rng, shape, cuts, smallest, largest):
    gain = 1.0
    for dim, shards_of in cuts:
        heights = jax.random.uniform(jax.random.fold_in(jax.random.fold_in(rng, 6), dim), (shards_of,), jnp.float32, smallest / len(cuts), largest / len(cuts))
        gain = gain * jnp.repeat(jnp.exp(heights), shape[dim] // shards_of).reshape((-1,) + (1,) * (len(shape) - 1 - dim))
    return gain


def noise(stream_key, shape, width, bound, shards=(), kind=jnp.bfloat16):
    values = width * jax.random.normal(stream_key, shape, jnp.float32)
    if shards:
        values = values * shard_levels(stream_key, shape, shards, -0.22, 0.18)
    return jnp.clip(values, -bound, bound).astype(kind)


def setup_inputs(seed: int = 0) -> dict:
    key_list = jax.random.split(jax.random.key(seed), 19)
    return {
        "residual": noise(key_list[0], (BATCH, LENGTH, D), 1.0, 6.0, ((0, 4), (1, 8))),
        "query": draw_query(jax.random.fold_in(key_list[18], 71), 0),
        "latent": noise(key_list[2], (BATCH, LENGTH, LATENT), 1.0, 6.0, ((0, 4), (1, 8))),
        "rope_key": draw_rope_key(jax.random.fold_in(key_list[18], 71), 0),
        "latent_gain": jnp.clip(1.0 + 0.18 * jax.random.normal(key_list[4], (LATENT,), jnp.float32), 0.1, 1.9),
        "query_gain": draw_query_gain(jax.random.fold_in(key_list[18], 71), 0),
        "key_gain": draw_key_gain(jax.random.fold_in(key_list[18], 71), 0),
        "key_weight": noise(key_list[7], (LATENT, HEADS * NOPE), LATENT ** -0.5, 0.375),
        "value_weight": noise(key_list[8], (LATENT, HEADS * VDIM), LATENT ** -0.5, 0.375),
        "mix_gain": jnp.clip(1.0 + 0.18 * jax.random.normal(key_list[9], (HEADS * VDIM,), jnp.float32), 0.1, 1.9),
        "out_weight": noise(key_list[10], (HEADS * VDIM, D), (HEADS * VDIM) ** -0.5, 0.1875),
        "ffn_gain": jnp.clip(1.0 + 0.18 * jax.random.normal(key_list[11], (D,), jnp.float32), 0.1, 1.9),
        "expert_choice": draw_expert_choice(jax.random.fold_in(key_list[18], 71), 0),
        "group_prob": jnp.clip(0.25 + 0.75 * jax.random.uniform(key_list[13], (BATCH, LENGTH), jnp.float32) ** shard_levels(key_list[13], (BATCH, LENGTH), ((0, 4), (1, 8)), -0.2, 0.2), 0.25, 1.0),
        "expert_prob": jnp.clip(0.05 + 0.95 * jax.random.uniform(key_list[14], (BATCH, LENGTH, TOP), jnp.float32) ** shard_levels(key_list[14], (BATCH, LENGTH, TOP), ((0, 4), (1, 8)), -0.2, 0.2), 0.05, 1.0),
        "gate_weight": noise(key_list[15], (EXPERTS, D, FF), D ** -0.5, 0.125, ((0, 32),)),
        "up_weight": noise(key_list[16], (EXPERTS, D, FF), D ** -0.5, 0.125, ((0, 32),)),
        "down_weight": noise(key_list[17], (EXPERTS, FF, D), FF ** -0.5, 0.25, ((0, 32),)),
    }


eps = 1e-06

def rms_scale(vector, gains):
    return vector * lax.rsqrt(lax.optimization_barrier(jnp.mean(vector * vector, axis=-1, keepdims=True)) + eps) * gains

def rotate(vector, phases):
    half_width = vector.shape[-1] // 2
    lower_half = vector[..., :half_width]
    upper_half = vector[..., half_width:]
    cos_table = jnp.cos(phases)
    sin_table = jnp.sin(phases)
    return jnp.concatenate([lower_half * cos_table - upper_half * sin_table, upper_half * cos_table + lower_half * sin_table], axis=-1)

def angles(offset, span_count, rope_width):
    position = (offset + jnp.arange(span_count, dtype=jnp.int32)).astype(jnp.float32)
    frequency = 10000.0 ** (-2.0 * jnp.arange(rope_width // 2, dtype=jnp.float32) / rope_width)
    return position[:, None] * frequency[None, :]

def head_vectors(nope_part, rope_part, gains, phases):
    normed_all = rms_scale(jnp.concatenate([nope_part, rope_part], axis=-1), gains)
    split_at = nope_part.shape[-1]
    turned = rotate(normed_all[..., split_at:], phases[:, None, :])
    return jnp.concatenate([normed_all[..., :split_at], turned], axis=-1).astype(jnp.bfloat16)

def attend_one(query_head, key_head, value_head):
    length = query_head.shape[0]
    blocks_count = max(4, length // 1024)
    block_rows = length // blocks_count
    score_scale = query_head.shape[-1] ** (-0.5)
    pieces = []
    for block_index in range(blocks_count):
        first_row = block_index * block_rows
        last_row = first_row + block_rows
        scores = jnp.dot(query_head[first_row:last_row], key_head[:last_row].T, preferred_element_type=jnp.float32) * score_scale
        query_pos = first_row + jnp.arange(block_rows, dtype=jnp.int32)
        key_pos = jnp.arange(last_row, dtype=jnp.int32)
        allowed = key_pos[None, :] // SPAN <= query_pos[:, None] // SPAN
        scores = jnp.where(allowed, scores, -1e+30)
        row_top = lax.optimization_barrier(jnp.max(scores, axis=-1, keepdims=True))
        raised = jnp.exp(scores - row_top)
        row_sum = lax.optimization_barrier(jnp.sum(raised, axis=-1))
        summed = jnp.dot(raised.astype(jnp.bfloat16), value_head[:last_row], preferred_element_type=jnp.float32)
        pieces.append((summed / row_sum[:, None]).astype(jnp.bfloat16))
    return jnp.concatenate(pieces, axis=0)

def reference(residual, query, latent, rope_key, latent_gain, query_gain, key_gain, key_weight, value_weight, mix_gain, out_weight, ffn_gain, expert_choice, group_prob, expert_prob, gate_weight, up_weight, down_weight):
    phases = angles(0, LENGTH, ROPE)
    raw_query = query.astype(jnp.float32).reshape(BATCH, LENGTH, HEADS, QK)
    queries = head_vectors(raw_query[..., :NOPE], raw_query[..., NOPE:], query_gain, phases)
    normed_latent = rms_scale(latent.astype(jnp.float32), latent_gain).astype(jnp.bfloat16)
    flat_latent = normed_latent.reshape(BATCH * LENGTH, LATENT)
    key_part = jnp.dot(flat_latent, key_weight, preferred_element_type=jnp.float32).astype(jnp.bfloat16)
    key_part = key_part.reshape(BATCH, LENGTH, HEADS, NOPE)
    values = jnp.dot(flat_latent, value_weight, preferred_element_type=jnp.float32).astype(jnp.bfloat16)
    values = values.reshape(BATCH, LENGTH, HEADS, VDIM)
    shared_rope = jnp.broadcast_to(rope_key.astype(jnp.float32)[:, :, None, :], (BATCH, LENGTH, HEADS, ROPE))
    keys = head_vectors(key_part.astype(jnp.float32), shared_rope, key_gain, phases)

    def arrange(array):
        return array.transpose(0, 2, 1, 3).reshape(BATCH * HEADS, LENGTH, array.shape[-1])

    def per_head(operands):
        return attend_one(operands[0], operands[1], operands[2])
    heads_out = lax.map(per_head, (arrange(queries), arrange(keys), arrange(values)))
    heads_out = heads_out.reshape(BATCH, HEADS, LENGTH, VDIM).transpose(0, 2, 1, 3).reshape(BATCH * LENGTH, HEADS * VDIM)
    mixed_in = rms_scale(heads_out.astype(jnp.float32), mix_gain).astype(jnp.bfloat16)
    stream = residual.reshape(BATCH * LENGTH, D).astype(jnp.float32) + jnp.dot(mixed_in, out_weight, preferred_element_type=jnp.float32)
    normed = rms_scale(stream, ffn_gain).astype(jnp.bfloat16)
    shares = expert_prob.reshape(BATCH * LENGTH, TOP)
    route_weight = group_prob.reshape(BATCH * LENGTH, 1) * shares / lax.optimization_barrier(jnp.sum(shares, axis=-1, keepdims=True))
    flat_choice = expert_choice.reshape(BATCH * LENGTH * TOP)
    flat_route = route_weight.reshape(BATCH * LENGTH * TOP)
    assignments = BATCH * LENGTH * TOP
    most_rows = CAP * N_SP * N_DP

    def serve_expert(running, operands):
        expert_id, gate_one, up_one, down_one = operands
        picked = jnp.nonzero(flat_choice == expert_id, size=most_rows, fill_value=assignments)[0].astype(jnp.int32)
        token_ids = picked // TOP
        rows_in = jnp.take(normed, token_ids, axis=0, mode='fill', fill_value=0)
        gate_act = jnp.dot(rows_in, gate_one, preferred_element_type=jnp.float32)
        upward = jnp.dot(rows_in, up_one, preferred_element_type=jnp.float32)
        hidden = (jax.nn.silu(gate_act) * upward).astype(jnp.bfloat16)
        expert_out = jnp.dot(hidden, down_one, preferred_element_type=jnp.float32).astype(jnp.bfloat16)
        weight_of = jnp.take(flat_route, picked, mode='fill', fill_value=0.0)
        running = running.at[token_ids].add(weight_of[:, None] * expert_out.astype(jnp.float32), mode='drop')
        return (running, None)
    start_sum = jnp.zeros((BATCH * LENGTH, D), jnp.float32)
    routed_sum, _ = lax.scan(serve_expert, start_sum, (jnp.arange(EXPERTS, dtype=jnp.int32), gate_weight, up_weight, down_weight))
    return (stream + routed_sum).astype(jnp.bfloat16).reshape(BATCH, LENGTH, D)
```

```python
import functools

import jax
import jax.numpy as jnp
from jax import lax
from jax.experimental import pallas as pl
from jax.experimental.pallas import tpu as pltpu
from jax.sharding import PartitionSpec as P

GROUPS = 4
SPAN = 64


eps = 1e-06


def angles(offset, span_count, rope_width):
    position = (offset + jnp.arange(span_count, dtype=jnp.int32)).astype(jnp.float32)
    frequency = 10000.0 ** (-2.0 * jnp.arange(rope_width // 2, dtype=jnp.float32) / rope_width)
    return position[:, None] * frequency[None, :]


def dot32(a, b):
    return jnp.dot(a, b, preferred_element_type=jnp.float32)


def dot_t(a, b):
    return lax.dot_general(a, b, (((0,), (0,)), ((), ())), preferred_element_type=jnp.float32)


def expert_kernel(
    n_y,
    n_dp,
    cap,
    rows,
    normed_ref,
    info_ref,
    pick_ref,
    stream_ref,
    gate_hbm,
    up_hbm,
    down_hbm,
    out_ref,
    gate_ref,
    up_ref,
    down_ref,
    notes_out,
    notes,
    out1,
    in1,
    out2,
    arrive,
    served,
    back2,
    merged,
    home,
    w_sem,
    s0,
    r0,
    s1,
    r1,
    s2,
    r2,
    s3,
    r3,
    s4,
    r4,
):
    bf = jnp.bfloat16
    peers = n_y * n_dp
    chunks = in1.shape[1]
    part = in1.shape[3]
    sp = lax.axis_index("sp")
    dp = lax.axis_index("dp")
    plane = sp // n_y
    row = sp % n_y
    mine = row * n_dp + dp

    def column(k):
        return {"sp": ((plane + k) % GROUPS) * n_y + row, "dp": dp}

    def peer(j):
        other = (mine + j) % peers
        return {"sp": plane * n_y + other // n_dp, "dp": other % n_dp}

    loads = [
        pltpu.make_async_copy(gate_hbm, gate_ref, w_sem.at[0]),
        pltpu.make_async_copy(up_hbm, up_ref, w_sem.at[1]),
        pltpu.make_async_copy(down_hbm, down_ref, w_sem.at[2]),
    ]
    for load in loads:
        load.start()
    barrier = pltpu.get_barrier_semaphore()
    for k in range(1, GROUPS):
        pl.semaphore_signal(barrier, inc=1, device_id=column(k), device_id_type=pl.DeviceIdType.MESH)
    for j in range(1, peers):
        pl.semaphore_signal(barrier, inc=1, device_id=peer(j), device_id_type=pl.DeviceIdType.MESH)

    def remote(src, dst, send, recv, target):
        return pltpu.make_async_remote_copy(
            src_ref=src,
            dst_ref=dst,
            send_sem=send,
            recv_sem=recv,
            device_id=target,
            device_id_type=pl.DeviceIdType.MESH,
        )

    send_first = 1 + (plane + 1) // 2
    send_last = GROUPS - 1 - 2 * (plane // 2)
    send_order = (send_first, 6 - send_first - send_last, send_last)
    recv_first = 6 - send_first - send_last
    recv_last = 1 + 2 * (plane % 2)
    recv_order = (recv_first, 6 - recv_first - recv_last, recv_last)

    def span(c):
        return slice(c * part, (c + 1) * part)

    def note(k):
        return remote(notes_out.at[k], notes.at[k], s0.at[k], r0.at[k], column(k))

    def first(k, c):
        return remote(out1.at[k, c], in1.at[k, c], s1.at[k, c], r1.at[k, c], column(k))

    def second(k, c, j):
        return remote(
            out2.at[k, c, (mine + j) % peers],
            arrive.at[k, c, j],
            s2.at[k, c, j],
            r2.at[k, c, j],
            peer(j),
        )

    def third(k, c, j):
        return remote(
            served.at[k, c, j],
            back2.at[k, c, mine],
            s3.at[k, c, j],
            r3.at[k, c, peers - j],
            peer(peers - j),
        )

    def fourth(k, c):
        return remote(merged.at[k, c], home.at[k, c], s4.at[k, c], r4.at[k, c], column(GROUPS - k))

    for i, k in enumerate(send_order):
        picks = pick_ref[(plane + k) % GROUPS]
        notes_out[k] = dot32(picks, info_ref[...]).astype(bf)
        for c in range(chunks):
            out1[k, c] = dot32(picks, normed_ref[:, span(c)]).astype(bf)
            if i == 0 and c == 0:
                pl.semaphore_wait(barrier, GROUPS - 1 + peers - 1)
            if c == 0:
                note(k).start()
            first(k, c).start()
    own = pick_ref[plane]
    notes[0] = dot32(own, info_ref[...]).astype(bf)
    for c in range(chunks):
        in1[0, c] = dot32(own, normed_ref[:, span(c)]).astype(bf)

    def slots(k):
        info = notes[k].astype(jnp.float32)
        place = lax.broadcasted_iota(jnp.int32, (rows, peers * cap), 1).astype(jnp.float32)
        return place == info[:, 0:1], place == info[:, 1:2], info

    def scatter(k, local):
        if not local:
            note(k).wait_recv()
        at0, at1, _ = slots(k)
        choose = (at0.astype(jnp.float32) + at1.astype(jnp.float32)).astype(bf)
        for c in range(chunks):
            if not local:
                first(k, c).wait_recv()
            placed = dot_t(choose, in1[k, c]).astype(bf)
            for e in range(peers):
                out2[k, c, e] = placed[e * cap : (e + 1) * cap]
            for j in range(1, peers):
                second(k, c, j).start()
            arrive[k, c, 0] = out2[k, c, mine]

    def serve(k, load):
        gate_act = None
        for c in range(chunks):
            for j in range(1, peers):
                second(k, c, j).wait_recv()
            if load and c == 0:
                for copy in loads:
                    copy.wait()
            given = arrive[k, c].reshape(peers * cap, part)
            gate_part = dot32(given, gate_ref[span(c), :])
            up_part = dot32(given, up_ref[span(c), :])
            gate_act = gate_part if gate_act is None else gate_act + gate_part
            upward = up_part if c == 0 else upward + up_part
        hidden = (gate_act * (1.0 / (1.0 + jnp.exp(-gate_act))) * upward).astype(bf)
        for c in range(chunks):
            result = dot32(hidden, down_ref[:, span(c)]).astype(bf)
            for j in range(peers):
                served[k, c, j] = result[j * cap : (j + 1) * cap]
            for j in range(1, peers):
                third(k, c, j).start()
            back2[k, c, mine] = served[k, c, 0]

    def merge(k, local):
        at0, at1, info = slots(k)
        high = jnp.where(at0, info[:, 2:3], 0.0) + jnp.where(at1, info[:, 4:5], 0.0)
        low = jnp.where(at0, info[:, 3:4], 0.0) + jnp.where(at1, info[:, 5:6], 0.0)
        high = high.astype(bf)
        low = low.astype(bf)
        for c in range(chunks):
            for j in range(1, peers):
                third(k, c, j).wait_recv()
            got = back2[k, c].reshape(peers * cap, part)
            total = (dot32(high, got) + dot32(low, got)).astype(bf)
            if local:
                home[0, c] = total
            else:
                merged[k, c] = total
                fourth(k, c).start()

    scatter(0, True)
    scatter(recv_order[0], False)
    serve(recv_order[0], True)
    serve(0, False)
    scatter(recv_order[1], False)
    merge(recv_order[0], False)
    serve(recv_order[1], False)
    scatter(recv_order[2], False)
    merge(recv_order[1], False)
    serve(recv_order[2], False)
    merge(0, True)
    merge(recv_order[2], False)
    for c in range(chunks):
        total = stream_ref[:, span(c)] + dot_t(own, home[0, c])
        for k in send_order:
            fourth(k, c).wait_recv()
            total = total + dot_t(pick_ref[(plane + k) % GROUPS], home[k, c])
        out_ref[:, span(c)] = total.astype(bf)
    for k in range(GROUPS):
        if k:
            note(k).wait_send()
        for c in range(chunks):
            if k:
                first(k, c).wait_send()
                fourth(k, c).wait_send()
            for j in range(1, peers):
                second(k, c, j).wait_send()
                third(k, c, j).wait_send()


def attention_kernel(
    n_sp,
    n_y,
    heads,
    nope,
    rope,
    value_width,
    query_ref,
    packed_ref,
    latent_gain_ref,
    query_gain_ref,
    query_swap_ref,
    key_gain_ref,
    key_swap_ref,
    cos_ref,
    sin_ref,
    key_weight_ref,
    value_weight_ref,
    residual_ref,
    mix_gain_ref,
    ffn_gain_ref,
    out_weight_hbm,
    stream_ref,
    normed_ref,
    out_weight_ref,
    queries_in,
    packed_in,
    queries,
    keys,
    values,
    heads_out,
    token_in,
    mixed,
    w_sem,
    sq,
    rq,
    sz,
    rz,
    sy,
    ry,
    so,
    ro,
):
    bf = jnp.bfloat16
    tok = residual_ref.shape[0]
    length = n_sp * tok
    qk = nope + rope
    lat = packed_ref.shape[1]
    me = lax.axis_index("sp")
    plane = me // n_y
    row = me % n_y
    load = pltpu.make_async_copy(out_weight_hbm, out_weight_ref, w_sem.at[0])
    load.start()

    def remote(src, dst, send, recv, target):
        return pltpu.make_async_remote_copy(
            src_ref=src,
            dst_ref=dst,
            send_sem=send,
            recv_sem=recv,
            device_id={"sp": target},
            device_id_type=pl.DeviceIdType.MESH,
        )

    barrier = pltpu.get_barrier_semaphore()
    for j in range(1, n_sp):
        pl.semaphore_signal(
            barrier,
            inc=1,
            device_id={"sp": (me + j) % n_sp},
            device_id_type=pl.DeviceIdType.MESH,
        )
    pl.semaphore_wait(barrier, n_sp - 1)

    down = []
    for k in range(1, GROUPS):
        target = ((plane + k) % GROUPS) * n_y + row
        down.append(remote(packed_ref, packed_in.at[me], sz.at[k], rz.at[k], target))
        down[-1].start()
    across = []

    def spread(k, source):
        index = ((plane + GROUPS - k) % GROUPS) * n_y + row
        for m in range(1, n_y):
            target = plane * n_y + (row + m) % n_y
            across.append(remote(source, packed_in.at[index], sy.at[k, m], ry.at[k, m], target))
            across[-1].start()

    spread(0, packed_ref)
    sent = []
    for j in range(1, n_sp):
        target = (me + j) % n_sp
        sent.append(remote(query_ref.at[target], queries_in.at[me], sq.at[j], rq.at[j], target))
        sent[-1].start()
    packed_in[me] = packed_ref[...]
    queries_in[me] = query_ref[me]
    for k in range(1, GROUPS):
        down[k - 1].wait_recv()
        spread(k, packed_in.at[((plane + GROUPS - k) % GROUPS) * n_y + row])
    for copy in across:
        copy.wait_recv()

    def selector(rows, columns, source):
        i = lax.broadcasted_iota(jnp.int32, (rows, columns), 0)
        c = lax.broadcasted_iota(jnp.int32, (rows, columns), 1)
        return (i == source(c)).astype(jnp.float32).astype(bf)

    half = rope // 2

    def swapped(c):
        return jnp.where(c < nope, -1, jnp.where(c < nope + half, c + half, c - half))

    def shape_head(plain, turned, gain, swap_gain, rows):
        scale = lax.rsqrt(jnp.sum(plain * plain, axis=-1, keepdims=True) / qk + eps)
        return (
            plain * scale * gain * cos_ref[rows, :] + turned * scale * swap_gain * sin_ref[rows, :]
        ).astype(bf)

    strips = lat // rope
    strip_rows = tok // strips

    def prepare(s, carry):
        rows = pl.ds(pl.multiple_of(s * tok, tok), tok)
        block = packed_in[s]
        raw = block[:tok].astype(jnp.float32)
        scale = lax.rsqrt(jnp.mean(raw * raw, axis=-1, keepdims=True) + eps)
        latent = (raw * scale * latent_gain_ref[...]).astype(bf)
        values[rows, :] = dot32(latent, value_weight_ref[...]).astype(bf)
        part = dot32(latent, key_weight_ref[...]).astype(bf)
        tail = block[tok:]
        plain_rope = jnp.concatenate(
            [
                dot32(tail, selector(lat, qk, lambda c: jnp.where(c < nope, -1, c - nope + i * rope)))
                for i in range(strips)
            ],
            axis=0,
        )
        turned = jnp.concatenate(
            [
                dot32(
                    tail,
                    selector(
                        lat, qk, lambda c: jnp.where(c < nope, -1, swapped(c) - nope + i * rope)
                    ),
                )
                for i in range(strips)
            ],
            axis=0,
        )
        for h in range(heads):
            plain = plain_rope + dot32(
                part, selector(heads * nope, qk, lambda c: jnp.where(c < nope, c + h * nope, -1))
            )
            keys[h, rows, :] = shape_head(
                plain, turned, key_gain_ref[...], key_swap_ref[...], rows
            )
        return carry

    lax.fori_loop(0, n_sp, prepare, 0)
    for copy in sent:
        copy.wait_recv()

    def prepare_queries(s, carry):
        rows = pl.ds(pl.multiple_of(s * tok, tok), tok)
        raw = queries_in[s]
        for h in range(heads):
            plain = dot32(raw, selector(heads * qk, qk, lambda c: c + h * qk))
            turned = dot32(
                raw,
                selector(
                    heads * qk, qk, lambda c: jnp.where(c < nope, -1, swapped(c) + h * qk)
                ),
            )
            queries[h, rows, :] = shape_head(
                plain, turned, query_gain_ref[...], query_swap_ref[...], rows
            )
        return carry

    lax.fori_loop(0, n_sp, prepare_queries, 0)

    blocks = 4
    block_rows = length // blocks
    for b in range(blocks):
        first_row = b * block_rows
        last_row = first_row + block_rows
        total = None
        lane = lax.broadcasted_iota(jnp.int32, (block_rows, heads * value_width), 1)
        q_pos = first_row + lax.broadcasted_iota(jnp.int32, (block_rows, last_row), 0)
        k_pos = lax.broadcasted_iota(jnp.int32, (block_rows, last_row), 1)
        allowed = k_pos // SPAN <= q_pos // SPAN
        for h in range(heads):
            scores = lax.dot_general(
                queries[h, first_row:last_row],
                keys[h, :last_row],
                (((1,), (1,)), ((), ())),
                preferred_element_type=jnp.float32,
            ) * (qk ** (-0.5))
            scores = jnp.where(allowed, scores, -1e30)
            raised = jnp.exp(scores - jnp.max(scores, axis=-1, keepdims=True))
            row_sum = jnp.sum(raised, axis=-1, keepdims=True)
            mine = dot32(raised.astype(bf), values[:last_row]) / row_sum
            total = mine if total is None else jnp.where(lane < h * value_width, total, mine)
        total = total.astype(bf)
        for t in range(block_rows // tok):
            index = first_row // tok + t
            heads_out[index] = total[t * tok : (t + 1) * tok]

            @pl.when(index != me)
            def _():
                remote(
                    heads_out.at[index], token_in.at[me], so.at[index], ro.at[me], index
                ).start()

    token_in[me] = heads_out[me]
    load.wait()
    for j in range(1, n_sp):
        other = (me + j) % n_sp
        remote(
            heads_out.at[other], token_in.at[other], so.at[other], ro.at[other], other
        ).wait()
    wide = heads * value_width
    square = None
    for s in range(n_sp):
        piece = token_in[s].astype(jnp.float32)
        part = jnp.sum(piece * piece, axis=-1, keepdims=True)
        square = part if square is None else square + part
    scale = lax.rsqrt(square / (n_sp * wide) + eps)
    for s in range(n_sp):
        span = slice(s * wide, (s + 1) * wide)
        mixed[:, span] = (token_in[s].astype(jnp.float32) * scale * mix_gain_ref[:, span]).astype(bf)
    stream = residual_ref[...].astype(jnp.float32) + dot32(mixed[...], out_weight_ref[...])
    stream_ref[...] = stream
    scale = lax.rsqrt(jnp.mean(stream * stream, axis=-1, keepdims=True) + eps)
    normed_ref[...] = (stream * scale * ffn_gain_ref[...]).astype(bf)
    for copy in down + across + sent:
        copy.wait_send()


def attended(
    residual,
    query,
    latent,
    rope_key,
    latent_gain,
    query_gain,
    key_gain,
    key_weight,
    value_weight,
    mix_gain,
    out_weight,
    ffn_gain,
    head_count,
    nope,
    value_width,
):
    n_sp = lax.axis_size("sp")
    n_y = n_sp // GROUPS
    me = lax.axis_index("sp")
    tok, width = residual.shape
    rope = rope_key.shape[1]
    qk = nope + rope
    lat = latent.shape[1]
    heads = head_count // n_sp
    length = n_sp * tok
    half = rope // 2
    bf = jnp.bfloat16
    query_blocks = query.reshape(tok, n_sp, heads * qk).transpose(1, 0, 2)
    strips = lat // rope
    tail = rope_key.reshape(strips, tok // strips, rope).transpose(1, 0, 2).reshape(-1, lat)
    packed = jnp.concatenate([latent, tail], axis=0)
    phases = angles(0, length, rope)
    cos, sin = jnp.cos(phases), jnp.sin(phases)
    cos = jnp.concatenate([jnp.ones((length, nope), jnp.float32), cos, cos], axis=1)
    sin = jnp.concatenate([jnp.zeros((length, nope), jnp.float32), -sin, sin], axis=1)

    def swap(gain):
        return jnp.concatenate([gain[:nope], gain[nope + half :], gain[nope : nope + half]])

    key_own = lax.dynamic_slice_in_dim(key_weight, me * heads * nope, heads * nope, 1)
    value_own = lax.dynamic_slice_in_dim(value_weight, me * heads * value_width, heads * value_width, 1)
    vmem = pl.BlockSpec(memory_space=pltpu.VMEM)
    dma = pltpu.SemaphoreType.DMA
    wide = heads * value_width
    return pl.pallas_call(
        functools.partial(attention_kernel, n_sp, n_y, heads, nope, rope, value_width),
        out_shape=(
            jax.ShapeDtypeStruct((tok, width), jnp.float32),
            jax.ShapeDtypeStruct((tok, width), bf),
        ),
        in_specs=[vmem] * 14 + [pl.BlockSpec(memory_space=pl.ANY)],
        out_specs=(vmem, vmem),
        scratch_shapes=[
            pltpu.VMEM(out_weight.shape, bf),
            pltpu.VMEM((n_sp, tok, heads * qk), bf),
            pltpu.VMEM((n_sp,) + packed.shape, bf),
            pltpu.VMEM((heads, length, qk), bf),
            pltpu.VMEM((heads, length, qk), bf),
            pltpu.VMEM((length, wide), bf),
            pltpu.VMEM((n_sp, tok, wide), bf),
            pltpu.VMEM((n_sp, tok, wide), bf),
            pltpu.VMEM((tok, n_sp * wide), bf),
            dma((1,)),
            dma((n_sp,)),
            dma((n_sp,)),
            dma((GROUPS,)),
            dma((GROUPS,)),
            dma((GROUPS, n_y)),
            dma((GROUPS, n_y)),
            dma((n_sp,)),
            dma((n_sp,)),
        ],
        compiler_params=pltpu.CompilerParams(
            collective_id=1, has_side_effects=True, vmem_limit_bytes=48 * 1024 * 1024
        ),
    )(
        query_blocks,
        packed,
        latent_gain[None],
        query_gain[None],
        swap(query_gain)[None],
        key_gain[None],
        swap(key_gain)[None],
        cos,
        sin,
        key_own,
        value_own,
        residual,
        mix_gain[None],
        ffn_gain[None],
        out_weight,
    )


def routed(normed, stream, choice, group_prob, share, gate, up, down, expert_total):
    tok_rows, width = normed.shape
    n_y = lax.axis_size("sp") // GROUPS
    n_dp = lax.axis_size("dp")
    per_group = expert_total // GROUPS
    cap = tok_rows * GROUPS // expert_total
    rows = per_group * cap // choice.shape[1]
    group = choice[:, 0] // per_group
    order = jnp.arange(tok_rows, dtype=jnp.int32)
    before = order[None, :] < order[:, None]
    rank = jnp.sum((before & (group[None, :] == group[:, None])).astype(jnp.int32), axis=1)
    line = group * rows + rank
    pick = (
        (line[None, :] == jnp.arange(GROUPS * rows, dtype=jnp.int32)[:, None])
        .astype(jnp.bfloat16)
        .reshape(GROUPS, rows, tok_rows)
    )
    route = group_prob[:, None] * share / jnp.sum(share, axis=-1, keepdims=True)
    earlier = jnp.sum(
        (
            before[:, None, :, None] & (choice[:, :, None, None] == choice[None, None, :, :])
        ).astype(jnp.int32),
        axis=(2, 3),
    )
    position = (choice - group[:, None] * per_group) * cap + earlier
    high = lax.reduce_precision(route, 8, 7)
    low = route - high
    columns = jnp.concatenate(
        [
            position.astype(jnp.float32),
            jnp.stack([high[:, 0], low[:, 0], high[:, 1], low[:, 1]], axis=1),
            jnp.zeros((tok_rows, 122), jnp.float32),
        ],
        axis=1,
    ).astype(jnp.bfloat16)
    hidden = gate.shape[1]
    chunks = 4
    part = width // chunks
    bf = jnp.bfloat16
    vmem = pl.BlockSpec(memory_space=pltpu.VMEM)
    hbm = pl.BlockSpec(memory_space=pl.ANY)
    dma = pltpu.SemaphoreType.DMA
    return pl.pallas_call(
        functools.partial(expert_kernel, n_y, n_dp, cap, rows),
        out_shape=jax.ShapeDtypeStruct((tok_rows, width), bf),
        in_specs=[vmem] * 4 + [hbm] * 3,
        out_specs=vmem,
        scratch_shapes=[
            pltpu.VMEM((width, hidden), bf),
            pltpu.VMEM((width, hidden), bf),
            pltpu.VMEM((hidden, width), bf),
            pltpu.VMEM((GROUPS, rows, 128), bf),
            pltpu.VMEM((GROUPS, rows, 128), bf),
            pltpu.VMEM((GROUPS, chunks, rows, part), bf),
            pltpu.VMEM((GROUPS, chunks, rows, part), bf),
            pltpu.VMEM((GROUPS, chunks, per_group, cap, part), bf),
            pltpu.VMEM((GROUPS, chunks, per_group, cap, part), bf),
            pltpu.VMEM((GROUPS, chunks, per_group, cap, part), bf),
            pltpu.VMEM((GROUPS, chunks, per_group, cap, part), bf),
            pltpu.VMEM((GROUPS, chunks, rows, part), bf),
            pltpu.VMEM((GROUPS, chunks, rows, part), bf),
            dma((3,)),
            dma((GROUPS,)),
            dma((GROUPS,)),
            dma((GROUPS, chunks)),
            dma((GROUPS, chunks)),
            dma((GROUPS, chunks, per_group)),
            dma((GROUPS, chunks, per_group)),
            dma((GROUPS, chunks, per_group)),
            dma((GROUPS, chunks, per_group)),
            dma((GROUPS, chunks)),
            dma((GROUPS, chunks)),
        ],
        compiler_params=pltpu.CompilerParams(
            collective_id=0, has_side_effects=True, vmem_limit_bytes=60 * 1024 * 1024
        ),
    )(normed, columns, pick, stream, gate, up, down)


def per_device(
    residual,
    query,
    latent,
    rope_key,
    latent_gain,
    query_gain,
    key_gain,
    key_weight,
    value_weight,
    mix_gain,
    out_weight,
    ffn_gain,
    expert_choice,
    group_prob,
    expert_prob,
    gate_weight,
    up_weight,
    down_weight,
):
    rope_width = rope_key.shape[2]
    qk_width = query_gain.shape[0]
    nope_width = qk_width - rope_width
    head_count = query.shape[2] // qk_width
    value_width = value_weight.shape[1] // head_count
    seq_devices = lax.axis_size("sp")
    stream, normed = attended(
        residual[0],
        query[0],
        latent[0],
        rope_key[0],
        latent_gain,
        query_gain,
        key_gain,
        key_weight,
        value_weight,
        mix_gain,
        out_weight,
        ffn_gain,
        head_count,
        nope_width,
        value_width,
    )
    expert_total = seq_devices * lax.axis_size("dp")
    return routed(
        normed,
        stream,
        expert_choice[0],
        group_prob[0],
        expert_prob[0],
        gate_weight[0],
        up_weight[0],
        down_weight[0],
        expert_total,
    )[None]


def solution(mesh):
    return jax.shard_map(
        per_device,
        mesh=mesh,
        in_specs=(
            P("dp", "sp", None),
            P("dp", "sp", None),
            P("dp", "sp", None),
            P("dp", "sp", None),
            P(),
            P(),
            P(),
            P(),
            P(),
            P(),
            P(),
            P(),
            P("dp", "sp", None),
            P("dp", "sp"),
            P("dp", "sp", None),
            P(("sp", "dp"), None, None),
            P(("sp", "dp"), None, None),
            P(("sp", "dp"), None, None),
        ),
        out_specs=P("dp", "sp", None),
        check_vma=False,
    )
```

```python
import functools

import jax
import jax.numpy as jnp
from jax import lax
from jax.experimental import pallas as pl
from jax.experimental.pallas import tpu as pltpu
from jax.sharding import PartitionSpec as P

GROUPS = 4
SPAN = 64


eps = 1e-06


def angles(offset, span_count, rope_width):
    position = (offset + jnp.arange(span_count, dtype=jnp.int32)).astype(jnp.float32)
    frequency = 10000.0 ** (-2.0 * jnp.arange(rope_width // 2, dtype=jnp.float32) / rope_width)
    return position[:, None] * frequency[None, :]


def dot32(a, b):
    return jnp.dot(a, b, preferred_element_type=jnp.float32)


def dot_t(a, b):
    return lax.dot_general(a, b, (((0,), (0,)), ((), ())), preferred_element_type=jnp.float32)


def expert_kernel(
    n_y,
    n_dp,
    cap,
    rows,
    normed_ref,
    info_ref,
    pick_ref,
    stream_ref,
    gate_hbm,
    up_hbm,
    down_hbm,
    out_ref,
    gate_ref,
    up_ref,
    down_ref,
    notes_out,
    notes,
    out1,
    in1,
    out2,
    arrive,
    served,
    back2,
    merged,
    home,
    w_sem,
    s0,
    r0,
    s1,
    r1,
    s2,
    r2,
    s3,
    r3,
    s4,
    r4,
):
    bf = jnp.bfloat16
    peers = n_y * n_dp
    chunks = in1.shape[1]
    part = in1.shape[3]
    sp = lax.axis_index("sp")
    dp = lax.axis_index("dp")
    plane = sp // n_y
    row = sp % n_y
    mine = row * n_dp + dp

    def column(k):
        return {"sp": ((plane + k) % GROUPS) * n_y + row, "dp": dp}

    def peer(j):
        other = (mine + j) % peers
        return {"sp": plane * n_y + other // n_dp, "dp": other % n_dp}

    loads = [
        pltpu.make_async_copy(gate_hbm, gate_ref, w_sem.at[0]),
        pltpu.make_async_copy(up_hbm, up_ref, w_sem.at[1]),
        pltpu.make_async_copy(down_hbm, down_ref, w_sem.at[2]),
    ]
    for load in loads:
        load.start()
    barrier = pltpu.get_barrier_semaphore()
    for k in range(1, GROUPS):
        pl.semaphore_signal(barrier, inc=1, device_id=column(k), device_id_type=pl.DeviceIdType.MESH)
    for j in range(1, peers):
        pl.semaphore_signal(barrier, inc=1, device_id=peer(j), device_id_type=pl.DeviceIdType.MESH)

    def remote(src, dst, send, recv, target):
        return pltpu.make_async_remote_copy(
            src_ref=src,
            dst_ref=dst,
            send_sem=send,
            recv_sem=recv,
            device_id=target,
            device_id_type=pl.DeviceIdType.MESH,
        )

    send_first = 1 + (plane + 1) // 2
    send_last = GROUPS - 1 - 2 * (plane // 2)
    send_order = (send_first, 6 - send_first - send_last, send_last)
    recv_first = 6 - send_first - send_last
    recv_last = 1 + 2 * (plane % 2)
    recv_order = (recv_first, 6 - recv_first - recv_last, recv_last)

    def span(c):
        return slice(c * part, (c + 1) * part)

    def note(k):
        return remote(notes_out.at[k], notes.at[k], s0.at[k], r0.at[k], column(k))

    def first(k, c):
        return remote(out1.at[k, c], in1.at[k, c], s1.at[k, c], r1.at[k, c], column(k))

    def second(k, c, j):
        return remote(
            out2.at[k, c, (mine + j) % peers],
            arrive.at[k, c, j],
            s2.at[k, c, j],
            r2.at[k, c, j],
            peer(j),
        )

    def third(k, c, j):
        return remote(
            served.at[k, c, j],
            back2.at[k, c, mine],
            s3.at[k, c, j],
            r3.at[k, c, peers - j],
            peer(peers - j),
        )

    def fourth(k, c):
        return remote(merged.at[k, c], home.at[k, c], s4.at[k, c], r4.at[k, c], column(GROUPS - k))

    for i, k in enumerate(send_order):
        picks = pick_ref[(plane + k) % GROUPS]
        notes_out[k] = dot32(picks, info_ref[...]).astype(bf)
        for c in range(chunks):
            out1[k, c] = dot32(picks, normed_ref[:, span(c)]).astype(bf)
            if i == 0 and c == 0:
                pl.semaphore_wait(barrier, GROUPS - 1 + peers - 1)
            if c == 0:
                note(k).start()
            first(k, c).start()
    own = pick_ref[plane]
    notes[0] = dot32(own, info_ref[...]).astype(bf)
    for c in range(chunks):
        in1[0, c] = dot32(own, normed_ref[:, span(c)]).astype(bf)

    def slots(k):
        info = notes[k].astype(jnp.float32)
        place = lax.broadcasted_iota(jnp.int32, (rows, peers * cap), 1).astype(jnp.float32)
        return place == info[:, 0:1], place == info[:, 1:2], info

    def scatter(k, local):
        if not local:
            note(k).wait_recv()
        at0, at1, _ = slots(k)
        choose = (at0.astype(jnp.float32) + at1.astype(jnp.float32)).astype(bf)
        for c in range(chunks):
            if not local:
                first(k, c).wait_recv()
            placed = dot_t(choose, in1[k, c]).astype(bf)
            for e in range(peers):
                out2[k, c, e] = placed[e * cap : (e + 1) * cap]
            for j in range(1, peers):
                second(k, c, j).start()
            arrive[k, c, 0] = out2[k, c, mine]

    def serve(k, load):
        gate_act = None
        for c in range(chunks):
            for j in range(1, peers):
                second(k, c, j).wait_recv()
            if load and c == 0:
                for copy in loads:
                    copy.wait()
            given = arrive[k, c].reshape(peers * cap, part)
            gate_part = dot32(given, gate_ref[span(c), :])
            up_part = dot32(given, up_ref[span(c), :])
            gate_act = gate_part if gate_act is None else gate_act + gate_part
            upward = up_part if c == 0 else upward + up_part
        hidden = (gate_act * (1.0 / (1.0 + jnp.exp(-gate_act))) * upward).astype(bf)
        for c in range(chunks):
            result = dot32(hidden, down_ref[:, span(c)]).astype(bf)
            for j in range(peers):
                served[k, c, j] = result[j * cap : (j + 1) * cap]
            for j in range(1, peers):
                third(k, c, j).start()
            back2[k, c, mine] = served[k, c, 0]

    def merge(k, local):
        at0, at1, info = slots(k)
        high = jnp.where(at0, info[:, 2:3], 0.0) + jnp.where(at1, info[:, 4:5], 0.0)
        low = jnp.where(at0, info[:, 3:4], 0.0) + jnp.where(at1, info[:, 5:6], 0.0)
        high = high.astype(bf)
        low = low.astype(bf)
        for c in range(chunks):
            for j in range(1, peers):
                third(k, c, j).wait_recv()
            got = back2[k, c].reshape(peers * cap, part)
            total = (dot32(high, got) + dot32(low, got)).astype(bf)
            if local:
                home[0, c] = total
            else:
                merged[k, c] = total
                fourth(k, c).start()

    scatter(0, True)
    scatter(recv_order[0], False)
    scatter(recv_order[1], False)
    serve(recv_order[0], True)
    serve(recv_order[1], False)
    merge(recv_order[0], False)
    scatter(recv_order[2], False)
    merge(recv_order[1], False)
    serve(recv_order[2], False)
    serve(0, False)
    merge(recv_order[2], False)
    merge(0, True)
    for c in range(chunks):
        total = stream_ref[:, span(c)] + dot_t(own, home[0, c])
        for k in send_order:
            fourth(k, c).wait_recv()
            total = total + dot_t(pick_ref[(plane + k) % GROUPS], home[k, c])
        out_ref[:, span(c)] = total.astype(bf)
    for k in range(GROUPS):
        if k:
            note(k).wait_send()
        for c in range(chunks):
            if k:
                first(k, c).wait_send()
                fourth(k, c).wait_send()
            for j in range(1, peers):
                second(k, c, j).wait_send()
                third(k, c, j).wait_send()


def attention_kernel(
    n_sp,
    n_y,
    heads,
    nope,
    rope,
    value_width,
    query_ref,
    latent_ref,
    rope_ref,
    latent_gain_ref,
    gain_ref,
    rope_gain_ref,
    trig_ref,
    residual_ref,
    mix_gain_ref,
    ffn_gain_ref,
    key_weight_hbm,
    value_weight_hbm,
    out_weight_hbm,
    stream_ref,
    normed_ref,
    key_weight_ref,
    value_weight_ref,
    out_weight_ref,
    turned,
    packed,
    queries,
    values,
    top,
    acc,
    heads_out,
    w_sem,
    sz,
    rz,
    sy,
    ry,
):
    bf = jnp.bfloat16
    f32 = jnp.float32
    tok = residual_ref.shape[0]
    qk = nope + rope
    half = rope // 2
    lat = latent_ref.shape[1]
    wide = 2 * value_width
    chunk = n_y * tok
    me = lax.axis_index("sp")
    plane = me // n_y
    row = me % n_y
    loads = [
        pltpu.make_async_copy(key_weight_hbm, key_weight_ref, w_sem.at[0]),
        pltpu.make_async_copy(value_weight_hbm, value_weight_ref, w_sem.at[1]),
        pltpu.make_async_copy(out_weight_hbm, out_weight_ref, w_sem.at[2]),
    ]
    for load in loads:
        load.start()

    def at(index_plane, index_row):
        return {"sp": index_plane * n_y + index_row}

    barrier = pltpu.get_barrier_semaphore()
    for k in range(1, GROUPS):
        pl.semaphore_signal(
            barrier,
            inc=1,
            device_id=at((plane + k) % GROUPS, row),
            device_id_type=pl.DeviceIdType.MESH,
        )
    for m in range(1, n_y):
        pl.semaphore_signal(
            barrier,
            inc=1,
            device_id=at(plane, (row + m) % n_y),
            device_id_type=pl.DeviceIdType.MESH,
        )

    def remote(src, dst, send, recv, target):
        return pltpu.make_async_remote_copy(
            src_ref=src,
            dst_ref=dst,
            send_sem=send,
            recv_sem=recv,
            device_id=target,
            device_id_type=pl.DeviceIdType.MESH,
        )

    def up(k):
        return remote(
            packed.at[me], packed.at[me], sz.at[k], rz.at[k], at((plane + k) % GROUPS, row)
        )

    def across(k, m):
        index = ((plane + GROUPS - k) % GROUPS) * n_y + row
        return remote(
            packed.at[index],
            packed.at[index],
            sy.at[k, m],
            ry.at[k, m],
            at(plane, (row + m) % n_y),
        )

    raw = latent_ref[...].astype(f32)
    scale = lax.rsqrt(jnp.mean(raw * raw, axis=-1, keepdims=True) + eps)
    turned[...] = jnp.zeros(turned.shape, f32)
    turned[:, :rope] = rope_ref[...].astype(f32)
    tail = turned[...].T
    packed[me, :tok] = (raw * scale * latent_gain_ref[...]).astype(bf)
    packed[me, tok:, :tok] = tail[:half].astype(bf)
    packed[me, tok:, tok : 2 * tok] = tail[half:rope].astype(bf)
    pl.semaphore_wait(barrier, GROUPS - 1 + n_y - 1)
    send_first = 1 + (plane + 1) // 2
    send_last = GROUPS - 1 - 2 * (plane // 2)
    for k in (send_first, 6 - send_first - send_last, send_last):

        @pl.when(plane + k < GROUPS)
        def _():
            up(k).start()

    for m in range(1, n_y):
        across(0, m).start()

    def positions(first, count):
        span = pl.ds(pl.multiple_of(first * tok, tok), count)
        return trig_ref[:half, span], trig_ref[half:, span]

    cos, sin = positions(me, tok)
    pad = 128 - qk
    ones = jnp.ones((nope, tok), f32)
    none = jnp.zeros((half, tok), f32)
    empty = jnp.zeros((pad, tok), f32)
    zeros = jnp.zeros((nope, tok), f32)
    plain_table = jnp.concatenate([ones, cos, cos, empty], axis=0).T * gain_ref[0:1, :]
    lower_table = jnp.concatenate([zeros, -sin, none, empty], axis=0).T * gain_ref[1:2, :]
    upper_table = jnp.concatenate([zeros, none, sin, empty], axis=0).T * gain_ref[2:3, :]
    lane = lax.broadcasted_iota(jnp.int32, (tok, 128), 1)
    for h in range(heads):
        base = h * qk // 128 * 128
        shift = h * qk - base
        if shift + qk <= 128:
            x = query_ref[:, base : base + 128].astype(f32)
            if shift:
                x = pltpu.roll(x, 128 - shift, 1)
        else:
            x = query_ref[:, base : base + 256].astype(f32)
            x = pltpu.roll(x, 256 - shift, 1)[:, :128]
        x = jnp.where(lane < qk, x, 0.0)
        scale = lax.rsqrt(jnp.sum(x * x, axis=-1, keepdims=True) / qk + eps)
        y = (
            x * plain_table
            + pltpu.roll(x, 128 - half, 1) * lower_table
            + pltpu.roll(x, half, 1) * upper_table
        )
        queries[h] = (y * scale)[:, :qk].astype(bf)

    rope_low = rope_gain_ref[:half]
    rope_high = rope_gain_ref[half:]

    def attend(k, first):
        base = (plane - k) * n_y
        blocks = [packed[base + r] for r in range(n_y)]
        latents = jnp.concatenate([block[:tok] for block in blocks], axis=0)
        values[...] = dot32(latents, value_weight_ref[...]).astype(bf)
        part = lax.dot_general(
            key_weight_ref[...], latents, (((0,), (1,)), ((), ())), preferred_element_type=f32
        ).astype(bf)
        low = jnp.concatenate([block[tok:, :tok] for block in blocks], axis=1).astype(f32)
        high = jnp.concatenate([block[tok:, tok : 2 * tok] for block in blocks], axis=1).astype(f32)
        shared = jnp.sum(low * low + high * high, axis=0, keepdims=True)
        cos, sin = positions(base, chunk)
        low = low * rope_low
        high = high * rope_high
        rope_keys = jnp.concatenate([low * cos - high * sin, high * cos + low * sin], axis=0).astype(bf)
        if first:
            q_pos = row * tok + lax.broadcasted_iota(jnp.int32, (tok, chunk), 0)
            k_pos = lax.broadcasted_iota(jnp.int32, (tok, chunk), 1)
            allowed = k_pos // SPAN <= q_pos // SPAN
        for h in range(heads):
            own = part[h * nope : (h + 1) * nope]
            square = own.astype(f32)
            square = jnp.sum(square * square, axis=0, keepdims=True)
            scale = lax.rsqrt((square + shared) / qk + eps) * (qk ** (-0.5) * 1.4426950408889634)
            scores = dot32(queries[h], jnp.concatenate([own, rope_keys], axis=0)) * scale
            if first:
                scores = jnp.where(allowed, scores, -1e30)
            peak = jnp.max(scores, axis=-1, keepdims=True)
            if not first:
                before = top[h][:, 0:1]
                peak = jnp.maximum(before, peak)
            raised = jnp.exp2(scores - peak).astype(bf)
            pair = values[:, h // 2 * wide : (h // 2 + 1) * wide]
            lanes = lax.broadcasted_iota(jnp.int32, pair.shape, 1)
            mine = (lanes < value_width) if h % 2 == 0 else (lanes >= value_width)
            summed = dot32(raised, jnp.where(mine, pair, jnp.ones_like(pair)))
            if first:
                acc[h] = summed
            else:
                acc[h] = acc[h] * jnp.exp2(before - peak) + summed
            top[h] = jnp.broadcast_to(peak, top.shape[1:])

    loads[0].wait()
    loads[1].wait()

    def forward(k):
        up(k).wait_recv()
        for m in range(1, n_y):
            across(k, m).start()

    @pl.when(plane >= 1)
    def _():
        forward(1)

    for m in range(1, n_y):
        across(0, m).wait_recv()
    attend(0, True)

    def later(k, carry):
        @pl.when(plane >= k + 1)
        def _():
            forward(k + 1)

        for m in range(1, n_y):
            across(k, m).wait_recv()
        attend(k, False)
        return carry

    lax.fori_loop(1, plane + 1, later, 0)

    lanes = lax.broadcasted_iota(jnp.int32, (tok, wide), 1)
    square = None
    for p in range(heads // 2):
        even, odd = acc[2 * p], acc[2 * p + 1]
        total = jnp.where(lanes < value_width, odd, even)
        out = jnp.where(lanes < value_width, even, odd) / pltpu.roll(total, value_width, 1)
        out = out.astype(bf)
        heads_out[:, p * wide : (p + 1) * wide] = out
        out = out.astype(f32)
        part = jnp.sum(out * out, axis=-1, keepdims=True)
        square = part if square is None else square + part
    scale = lax.rsqrt(square / (heads * value_width) + eps)
    mixed = (heads_out[...].astype(f32) * scale * mix_gain_ref[...]).astype(bf)
    loads[2].wait()
    stream = residual_ref[...].astype(f32) + dot32(mixed, out_weight_ref[...])
    stream_ref[...] = stream
    scale = lax.rsqrt(jnp.mean(stream * stream, axis=-1, keepdims=True) + eps)
    normed_ref[...] = (stream * scale * ffn_gain_ref[...]).astype(bf)
    for m in range(1, n_y):
        across(0, m).wait_send()
    for k in range(1, GROUPS):

        @pl.when(plane + k < GROUPS)
        def _():
            up(k).wait_send()

        @pl.when(plane >= k)
        def _():
            for m in range(1, n_y):
                across(k, m).wait_send()


def attended(
    residual,
    query,
    latent,
    rope_key,
    latent_gain,
    query_gain,
    key_gain,
    key_weight,
    value_weight,
    mix_gain,
    out_weight,
    ffn_gain,
    head_count,
    nope,
    value_width,
):
    n_sp = lax.axis_size("sp")
    n_y = n_sp // GROUPS
    tok, width = residual.shape
    rope = rope_key.shape[1]
    qk = nope + rope
    lat = latent.shape[1]
    half = rope // 2
    bf = jnp.bfloat16
    phases = angles(0, n_sp * tok, rope).T
    trig = jnp.concatenate([jnp.cos(phases), jnp.sin(phases)], axis=0)
    zero = jnp.zeros((128 - qk,), jnp.float32)
    blank = jnp.zeros((nope,), jnp.float32)
    gap = jnp.zeros((half,), jnp.float32)
    own = query_gain * jnp.concatenate([key_gain[:nope], jnp.ones((rope,), jnp.float32)])
    gains = jnp.stack(
        [
            jnp.concatenate([own, zero]),
            jnp.concatenate([blank, query_gain[nope + half :], gap, zero]),
            jnp.concatenate([blank, gap, query_gain[nope : nope + half], zero]),
        ]
    )
    vmem = pl.BlockSpec(memory_space=pltpu.VMEM)
    hbm = pl.BlockSpec(memory_space=pl.ANY)
    dma = pltpu.SemaphoreType.DMA
    return pl.pallas_call(
        functools.partial(attention_kernel, n_sp, n_y, head_count, nope, rope, value_width),
        out_shape=(
            jax.ShapeDtypeStruct((tok, width), jnp.float32),
            jax.ShapeDtypeStruct((tok, width), bf),
        ),
        in_specs=[vmem] * 10 + [hbm] * 3,
        out_specs=(vmem, vmem),
        scratch_shapes=[
            pltpu.VMEM(key_weight.shape, bf),
            pltpu.VMEM(value_weight.shape, bf),
            pltpu.VMEM(out_weight.shape, bf),
            pltpu.VMEM((tok, 128), jnp.float32),
            pltpu.VMEM((n_sp, tok + half, lat), bf),
            pltpu.VMEM((head_count, tok, qk), bf),
            pltpu.VMEM((n_y * tok, head_count * value_width), bf),
            pltpu.VMEM((head_count, tok, 128), jnp.float32),
            pltpu.VMEM((head_count, tok, 2 * value_width), jnp.float32),
            pltpu.VMEM((tok, head_count * value_width), bf),
            dma((3,)),
            dma((GROUPS,)),
            dma((GROUPS,)),
            dma((GROUPS, n_y)),
            dma((GROUPS, n_y)),
        ],
        compiler_params=pltpu.CompilerParams(
            collective_id=1, has_side_effects=True, vmem_limit_bytes=48 * 1024 * 1024
        ),
    )(
        query,
        latent,
        rope_key,
        latent_gain[None],
        gains,
        key_gain[nope:, None],
        trig,
        residual,
        mix_gain[None],
        ffn_gain[None],
        key_weight,
        value_weight,
        out_weight,
    )


def routed(normed, stream, choice, group_prob, share, gate, up, down, expert_total):
    tok_rows, width = normed.shape
    n_y = lax.axis_size("sp") // GROUPS
    n_dp = lax.axis_size("dp")
    per_group = expert_total // GROUPS
    cap = tok_rows * GROUPS // expert_total
    rows = per_group * cap // choice.shape[1]
    group = choice[:, 0] // per_group
    order = jnp.arange(tok_rows, dtype=jnp.int32)
    before = order[None, :] < order[:, None]
    rank = jnp.sum((before & (group[None, :] == group[:, None])).astype(jnp.int32), axis=1)
    line = group * rows + rank
    pick = (
        (line[None, :] == jnp.arange(GROUPS * rows, dtype=jnp.int32)[:, None])
        .astype(jnp.bfloat16)
        .reshape(GROUPS, rows, tok_rows)
    )
    route = group_prob[:, None] * share / jnp.sum(share, axis=-1, keepdims=True)
    earlier = jnp.sum(
        (
            before[:, None, :, None] & (choice[:, :, None, None] == choice[None, None, :, :])
        ).astype(jnp.int32),
        axis=(2, 3),
    )
    position = (choice - group[:, None] * per_group) * cap + earlier
    high = lax.reduce_precision(route, 8, 7)
    low = route - high
    columns = jnp.concatenate(
        [
            position.astype(jnp.float32),
            jnp.stack([high[:, 0], low[:, 0], high[:, 1], low[:, 1]], axis=1),
            jnp.zeros((tok_rows, 122), jnp.float32),
        ],
        axis=1,
    ).astype(jnp.bfloat16)
    hidden = gate.shape[1]
    chunks = 4
    part = width // chunks
    bf = jnp.bfloat16
    vmem = pl.BlockSpec(memory_space=pltpu.VMEM)
    hbm = pl.BlockSpec(memory_space=pl.ANY)
    dma = pltpu.SemaphoreType.DMA
    return pl.pallas_call(
        functools.partial(expert_kernel, n_y, n_dp, cap, rows),
        out_shape=jax.ShapeDtypeStruct((tok_rows, width), bf),
        in_specs=[vmem] * 4 + [hbm] * 3,
        out_specs=vmem,
        scratch_shapes=[
            pltpu.VMEM((width, hidden), bf),
            pltpu.VMEM((width, hidden), bf),
            pltpu.VMEM((hidden, width), bf),
            pltpu.VMEM((GROUPS, rows, 128), bf),
            pltpu.VMEM((GROUPS, rows, 128), bf),
            pltpu.VMEM((GROUPS, chunks, rows, part), bf),
            pltpu.VMEM((GROUPS, chunks, rows, part), bf),
            pltpu.VMEM((GROUPS, chunks, per_group, cap, part), bf),
            pltpu.VMEM((GROUPS, chunks, per_group, cap, part), bf),
            pltpu.VMEM((GROUPS, chunks, per_group, cap, part), bf),
            pltpu.VMEM((GROUPS, chunks, per_group, cap, part), bf),
            pltpu.VMEM((GROUPS, chunks, rows, part), bf),
            pltpu.VMEM((GROUPS, chunks, rows, part), bf),
            dma((3,)),
            dma((GROUPS,)),
            dma((GROUPS,)),
            dma((GROUPS, chunks)),
            dma((GROUPS, chunks)),
            dma((GROUPS, chunks, per_group)),
            dma((GROUPS, chunks, per_group)),
            dma((GROUPS, chunks, per_group)),
            dma((GROUPS, chunks, per_group)),
            dma((GROUPS, chunks)),
            dma((GROUPS, chunks)),
        ],
        compiler_params=pltpu.CompilerParams(
            collective_id=0, has_side_effects=True, vmem_limit_bytes=60 * 1024 * 1024
        ),
    )(normed, columns, pick, stream, gate, up, down)


def per_device(
    residual,
    query,
    latent,
    rope_key,
    latent_gain,
    query_gain,
    key_gain,
    key_weight,
    value_weight,
    mix_gain,
    out_weight,
    ffn_gain,
    expert_choice,
    group_prob,
    expert_prob,
    gate_weight,
    up_weight,
    down_weight,
):
    rope_width = rope_key.shape[2]
    qk_width = query_gain.shape[0]
    nope_width = qk_width - rope_width
    head_count = query.shape[2] // qk_width
    value_width = value_weight.shape[1] // head_count
    seq_devices = lax.axis_size("sp")
    stream, normed = attended(
        residual[0],
        query[0],
        latent[0],
        rope_key[0],
        latent_gain,
        query_gain,
        key_gain,
        key_weight,
        value_weight,
        mix_gain,
        out_weight,
        ffn_gain,
        head_count,
        nope_width,
        value_width,
    )
    expert_total = seq_devices * lax.axis_size("dp")
    return routed(
        normed,
        stream,
        expert_choice[0],
        group_prob[0],
        expert_prob[0],
        gate_weight[0],
        up_weight[0],
        down_weight[0],
        expert_total,
    )[None]


def solution(mesh):
    return jax.shard_map(
        per_device,
        mesh=mesh,
        in_specs=(
            P("dp", "sp", None),
            P("dp", "sp", None),
            P("dp", "sp", None),
            P("dp", "sp", None),
            P(),
            P(),
            P(),
            P(),
            P(),
            P(),
            P(),
            P(),
            P("dp", "sp", None),
            P("dp", "sp"),
            P("dp", "sp", None),
            P(("sp", "dp"), None, None),
            P(("sp", "dp"), None, None),
            P(("sp", "dp"), None, None),
        ),
        out_specs=P("dp", "sp", None),
        check_vma=False,
    )
```

```python
import functools

import jax
import jax.numpy as jnp
from jax import lax
from jax.experimental import pallas as pl
from jax.experimental.pallas import tpu as pltpu
from jax.sharding import PartitionSpec as P

GROUPS = 4
SPAN = 64


eps = 1e-06


def angles(offset, span_count, rope_width):
    position = (offset + jnp.arange(span_count, dtype=jnp.int32)).astype(jnp.float32)
    frequency = 10000.0 ** (-2.0 * jnp.arange(rope_width // 2, dtype=jnp.float32) / rope_width)
    return position[:, None] * frequency[None, :]


def dot32(a, b):
    return jnp.dot(a, b, preferred_element_type=jnp.float32)


def dot_t(a, b):
    return lax.dot_general(a, b, (((0,), (0,)), ((), ())), preferred_element_type=jnp.float32)


def layer_kernel(
    n_sp,
    n_y,
    n_dp,
    heads,
    nope,
    rope,
    value_width,
    cap,
    rows,
    residual_hbm,
    query_hbm,
    latent_hbm,
    rope_hbm,
    latent_gain_hbm,
    query_gain_hbm,
    key_gain_hbm,
    cos_hbm,
    sin_hbm,
    mix_gain_hbm,
    ffn_gain_hbm,
    choice_hbm,
    group_prob_hbm,
    share_hbm,
    key_weight_hbm,
    value_weight_hbm,
    out_weight_hbm,
    gate_hbm,
    up_hbm,
    down_hbm,
    out_ref,
    residual_ref,
    query_ref,
    latent_ref,
    rope_ref,
    latent_gain_ref,
    query_gain_ref,
    key_gain_ref,
    cos_ref,
    sin_ref,
    mix_gain_ref,
    ffn_gain_ref,
    choice_ref,
    group_prob_ref,
    share_ref,
    key_weight_ref,
    value_weight_ref,
    out_weight_ref,
    gate_ref,
    up_ref,
    down_ref,
    gains,
    packed,
    queries,
    values,
    top,
    acc,
    heads_out,
    stream_ref,
    normed_ref,
    picks,
    notes_out,
    notes,
    out1,
    in1,
    out2,
    arrive,
    served,
    back2,
    merged,
    home,
    w_sem,
    sz,
    rz,
    sy,
    ry,
    s0,
    r0,
    s1,
    r1,
    s2,
    r2,
    s3,
    r3,
    s4,
    r4,
):
    bf = jnp.bfloat16
    f32 = jnp.float32
    tok = latent_ref.shape[0]
    qk = nope + rope
    half = rope // 2
    wide = 2 * value_width
    chunk = n_y * tok
    peers = n_y * n_dp
    chunks = in1.shape[1]
    part = in1.shape[3]
    me = lax.axis_index("sp")
    dp = lax.axis_index("dp")
    plane = me // n_y
    row = me % n_y
    mine = row * n_dp + dp

    def column(k):
        return {"sp": ((plane + k) % GROUPS) * n_y + row, "dp": dp}

    def peer(j):
        other = (mine + j) % peers
        return {"sp": plane * n_y + other // n_dp, "dp": other % n_dp}

    def at(index_plane, index_row):
        return {"sp": index_plane * n_y + index_row}

    barrier = pltpu.get_barrier_semaphore()
    for k in range(1, GROUPS):
        pl.semaphore_signal(barrier, inc=1, device_id=column(k), device_id_type=pl.DeviceIdType.MESH)
    for j in range(1, peers):
        pl.semaphore_signal(barrier, inc=1, device_id=peer(j), device_id_type=pl.DeviceIdType.MESH)

    pairs = (
        (latent_hbm, latent_ref),
        (latent_gain_hbm, latent_gain_ref),
        (rope_hbm, rope_ref),
        (choice_hbm, choice_ref),
        (group_prob_hbm, group_prob_ref),
        (share_hbm, share_ref),
        (query_gain_hbm, query_gain_ref),
        (key_gain_hbm, key_gain_ref),
        (cos_hbm, cos_ref),
        (sin_hbm, sin_ref),
        (query_hbm, query_ref),
        (key_weight_hbm, key_weight_ref),
        (value_weight_hbm, value_weight_ref),
        (residual_hbm, residual_ref),
        (mix_gain_hbm, mix_gain_ref),
        (ffn_gain_hbm, ffn_gain_ref),
        (out_weight_hbm, out_weight_ref),
        (gate_hbm, gate_ref),
        (up_hbm, up_ref),
        (down_hbm, down_ref),
    )
    copies = [
        (source, pltpu.make_async_copy(source, target, w_sem.at[i]))
        for i, (source, target) in enumerate(pairs)
    ]
    for _, copy in copies:
        copy.start()

    def ready(*sources):
        for source, copy in copies:
            if any(source is wanted for wanted in sources):
                copy.wait()

    def remote(src, dst, send, recv, target):
        return pltpu.make_async_remote_copy(
            src_ref=src,
            dst_ref=dst,
            send_sem=send,
            recv_sem=recv,
            device_id=target,
            device_id_type=pl.DeviceIdType.MESH,
        )

    def up(k):
        return remote(
            packed.at[me], packed.at[me], sz.at[k], rz.at[k], at((plane + k) % GROUPS, row)
        )

    def across(k, m):
        index = ((plane + GROUPS - k) % GROUPS) * n_y + row
        return remote(
            packed.at[index],
            packed.at[index],
            sy.at[k, m],
            ry.at[k, m],
            at(plane, (row + m) % n_y),
        )

    send_first = 1 + (plane + 1) // 2
    send_last = GROUPS - 1 - 2 * (plane // 2)
    send_order = (send_first, 6 - send_first - send_last, send_last)
    recv_first = 6 - send_first - send_last
    recv_last = 1 + 2 * (plane % 2)
    recv_order = (recv_first, 6 - recv_first - recv_last, recv_last)

    def span(c):
        return slice(c * part, (c + 1) * part)

    def note(k):
        return remote(notes_out.at[k], notes.at[k], s0.at[k], r0.at[k], column(k))

    def first(k, c):
        return remote(out1.at[k, c], in1.at[k, c], s1.at[k, c], r1.at[k, c], column(k))

    def second(k, c, j):
        return remote(
            out2.at[k, c, (mine + j) % peers],
            arrive.at[k, c, j],
            s2.at[k, c, j],
            r2.at[k, c, j],
            peer(j),
        )

    def third(k, c, j):
        return remote(
            served.at[k, c, j],
            back2.at[k, c, mine],
            s3.at[k, c, j],
            r3.at[k, c, peers - j],
            peer(peers - j),
        )

    def fourth(k, c):
        return remote(merged.at[k, c], home.at[k, c], s4.at[k, c], r4.at[k, c], column(GROUPS - k))

    ready(latent_hbm, latent_gain_hbm, rope_hbm)
    raw = latent_ref[...].astype(f32)
    scale = lax.rsqrt(jnp.mean(raw * raw, axis=-1, keepdims=True) + eps)
    packed[me, :tok] = (raw * scale * latent_gain_ref[...]).astype(bf)
    packed[me, tok:, :tok] = rope_ref[:half]
    packed[me, tok:, tok : 2 * tok] = rope_ref[half:]
    pl.semaphore_wait(barrier, GROUPS - 1 + peers - 1)
    for k in send_order:

        @pl.when(plane + k < GROUPS)
        def _():
            up(k).start()

    for m in range(1, n_y):
        across(0, m).start()

    def positions(first, count):
        span = pl.ds(pl.multiple_of(first * tok, tok), count)
        return cos_ref[:, span], sin_ref[:, span]

    ready(query_gain_hbm, key_gain_hbm, cos_hbm, sin_hbm)
    gains[...] = jnp.zeros(gains.shape, f32)
    gains[0:1, :qk] = query_gain_ref[...]
    gains[1:2, :qk] = key_gain_ref[...]
    both = gains[...]
    lane = lax.broadcasted_iota(jnp.int32, (1, 128), 1)
    plain_gain = both[0:1] * jnp.where(lane < nope, both[1:2], 1.0)
    lower_gain = pltpu.roll(both, 128 - half, 1)[0:1]
    upper_gain = pltpu.roll(both, half, 1)[0:1]
    key_gains = jnp.broadcast_to(both[1:2], (128, 128)).T
    rope_low = key_gains[nope : nope + half, 0:1]
    rope_high = key_gains[nope + half : qk, 0:1]
    ready(query_hbm)
    cos, sin = positions(me, tok)
    pad = 128 - qk
    ones = jnp.ones((nope, tok), f32)
    none = jnp.zeros((half, tok), f32)
    empty = jnp.zeros((pad, tok), f32)
    zeros = jnp.zeros((nope, tok), f32)
    plain_table = jnp.concatenate([ones, cos, cos, empty], axis=0).T * plain_gain
    lower_table = jnp.concatenate([zeros, -sin, none, empty], axis=0).T * lower_gain
    upper_table = jnp.concatenate([zeros, none, sin, empty], axis=0).T * upper_gain
    lane = lax.broadcasted_iota(jnp.int32, (tok, 128), 1)
    for h in range(heads):
        base = h * qk // 128 * 128
        shift = h * qk - base
        if shift + qk <= 128:
            x = query_ref[:, base : base + 128].astype(f32)
            if shift:
                x = pltpu.roll(x, 128 - shift, 1)
        else:
            x = query_ref[:, base : base + 256].astype(f32)
            x = pltpu.roll(x, 256 - shift, 1)[:, :128]
        x = jnp.where(lane < qk, x, 0.0)
        scale = lax.rsqrt(jnp.sum(x * x, axis=-1, keepdims=True) / qk + eps)
        y = (
            x * plain_table
            + pltpu.roll(x, 128 - half, 1) * lower_table
            + pltpu.roll(x, half, 1) * upper_table
        )
        queries[h] = (y * scale)[:, :qk].astype(bf)


    ready(choice_hbm, group_prob_hbm, share_hbm)
    per_group = peers
    group = choice_ref[0:1] // per_group
    order = lax.broadcasted_iota(jnp.int32, (tok, tok), 0)
    sooner = order < lax.broadcasted_iota(jnp.int32, (tok, tok), 1)

    def tall(line):
        return jnp.broadcast_to(line.astype(f32), (tok, tok)).T

    def count(flags):
        return jnp.sum(jnp.where(sooner & flags, 1.0, 0.0), axis=0, keepdims=True)

    rank = count(tall(group) == group.astype(f32))
    line = group.astype(f32) * rows + rank
    for g in range(GROUPS):
        slot = g * rows + lax.broadcasted_iota(jnp.int32, (rows, tok), 0)
        picks[g] = jnp.where(slot.astype(f32) == line, 1.0, 0.0).astype(bf)
    talls = (tall(choice_ref[0:1]), tall(choice_ref[1:2]))
    facts = []
    for s in range(2):
        named = choice_ref[s : s + 1].astype(f32)
        earlier = count(talls[0] == named) + count(talls[1] == named)
        facts.append((named - group.astype(f32) * per_group) * cap + earlier)
    total = share_ref[0:1] + share_ref[1:2]
    for s in range(2):
        route = group_prob_ref[...] * share_ref[s : s + 1] / total
        high = route.astype(bf).astype(f32)
        facts.append(high)
        facts.append(route - high)
    facts.append(jnp.zeros((128 - len(facts), tok), f32))
    facts = jnp.concatenate(facts, axis=0).astype(bf)

    def describe(g):
        return lax.dot_general(
            picks[g], facts, (((1,), (1,)), ((), ())), preferred_element_type=f32
        ).astype(bf)

    notes[0] = describe(plane)
    for k in send_order:
        notes_out[k] = describe((plane + k) % GROUPS)
        note(k).start()

    def attend(k, first):
        base = (plane - k) * n_y
        blocks = [packed[base + r] for r in range(n_y)]
        latents = jnp.concatenate([block[:tok] for block in blocks], axis=0)
        values[...] = dot32(latents, value_weight_ref[...]).astype(bf)
        part = lax.dot_general(
            key_weight_ref[...], latents, (((0,), (1,)), ((), ())), preferred_element_type=f32
        ).astype(bf)
        low = jnp.concatenate([block[tok:, :tok] for block in blocks], axis=1).astype(f32)
        high = jnp.concatenate([block[tok:, tok : 2 * tok] for block in blocks], axis=1).astype(f32)
        shared = jnp.sum(low * low + high * high, axis=0, keepdims=True)
        cos, sin = positions(base, chunk)
        low = low * rope_low
        high = high * rope_high
        rope_keys = jnp.concatenate([low * cos - high * sin, high * cos + low * sin], axis=0).astype(bf)
        if first:
            q_pos = row * tok + lax.broadcasted_iota(jnp.int32, (tok, chunk), 0)
            k_pos = lax.broadcasted_iota(jnp.int32, (tok, chunk), 1)
            allowed = k_pos // SPAN <= q_pos // SPAN
        for h in range(heads):
            own = part[h * nope : (h + 1) * nope]
            square = own.astype(f32)
            square = jnp.sum(square * square, axis=0, keepdims=True)
            scale = lax.rsqrt((square + shared) / qk + eps) * (qk ** (-0.5) * 1.4426950408889634)
            scores = dot32(queries[h], jnp.concatenate([own, rope_keys], axis=0)) * scale
            if first:
                scores = jnp.where(allowed, scores, -1e30)
            peak = jnp.max(scores, axis=-1, keepdims=True)
            if not first:
                before = top[h][:, 0:1]
                peak = jnp.maximum(before, peak)
            raised = jnp.exp2(scores - peak).astype(bf)
            pair = values[:, h // 2 * wide : (h // 2 + 1) * wide]
            lanes = lax.broadcasted_iota(jnp.int32, pair.shape, 1)
            mine = (lanes < value_width) if h % 2 == 0 else (lanes >= value_width)
            summed = dot32(raised, jnp.where(mine, pair, jnp.ones_like(pair)))
            if first:
                acc[h] = summed
            else:
                acc[h] = acc[h] * jnp.exp2(before - peak) + summed
            top[h] = jnp.broadcast_to(peak, top.shape[1:])

    ready(key_weight_hbm, value_weight_hbm)

    def forward(k):
        up(k).wait_recv()
        for m in range(1, n_y):
            across(k, m).start()

    @pl.when(plane >= 1)
    def _():
        forward(1)

    for m in range(1, n_y):
        across(0, m).wait_recv()
    attend(0, True)

    def later(k, carry):
        @pl.when(plane >= k + 1)
        def _():
            forward(k + 1)

        for m in range(1, n_y):
            across(k, m).wait_recv()
        attend(k, False)
        return carry

    lax.fori_loop(1, plane + 1, later, 0)

    lanes = lax.broadcasted_iota(jnp.int32, (tok, wide), 1)
    square = None
    for p in range(heads // 2):
        even, odd = acc[2 * p], acc[2 * p + 1]
        total = jnp.where(lanes < value_width, odd, even)
        out = jnp.where(lanes < value_width, even, odd) / pltpu.roll(total, value_width, 1)
        out = out.astype(bf)
        heads_out[:, p * wide : (p + 1) * wide] = out
        out = out.astype(f32)
        term = jnp.sum(out * out, axis=-1, keepdims=True)
        square = term if square is None else square + term
    scale = lax.rsqrt(square / (heads * value_width) + eps)
    ready(mix_gain_hbm)
    mixed = (heads_out[...].astype(f32) * scale * mix_gain_ref[...]).astype(bf)
    ready(residual_hbm, ffn_gain_hbm, out_weight_hbm)
    stream = residual_ref[...].astype(f32) + dot32(mixed, out_weight_ref[...])
    stream_ref[...] = stream
    scale = lax.rsqrt(jnp.mean(stream * stream, axis=-1, keepdims=True) + eps)
    normed_ref[...] = (stream * scale * ffn_gain_ref[...]).astype(bf)
    for k in send_order:
        chosen = picks[(plane + k) % GROUPS]
        for c in range(chunks):
            out1[k, c] = dot32(chosen, normed_ref[:, span(c)]).astype(bf)
            first(k, c).start()
    own = picks[plane]
    for c in range(chunks):
        in1[0, c] = dot32(own, normed_ref[:, span(c)]).astype(bf)

    def slots(k):
        info = notes[k].astype(jnp.float32)
        place = lax.broadcasted_iota(jnp.int32, (rows, peers * cap), 1).astype(jnp.float32)
        return place == info[:, 0:1], place == info[:, 1:2], info

    def scatter(k, local):
        if not local:
            note(k).wait_recv()
        at0, at1, _ = slots(k)
        choose = (at0.astype(jnp.float32) + at1.astype(jnp.float32)).astype(bf)
        for c in range(chunks):
            if not local:
                first(k, c).wait_recv()
            placed = dot_t(choose, in1[k, c]).astype(bf)
            for e in range(peers):
                out2[k, c, e] = placed[e * cap : (e + 1) * cap]
            for j in range(1, peers):
                second(k, c, j).start()
            arrive[k, c, 0] = out2[k, c, mine]

    def serve(k, load):
        gate_act = None
        for c in range(chunks):
            for j in range(1, peers):
                second(k, c, j).wait_recv()
            if load and c == 0:
                ready(gate_hbm, up_hbm, down_hbm)
            given = arrive[k, c].reshape(peers * cap, part)
            gate_part = dot32(given, gate_ref[span(c), :])
            up_part = dot32(given, up_ref[span(c), :])
            gate_act = gate_part if gate_act is None else gate_act + gate_part
            upward = up_part if c == 0 else upward + up_part
        hidden = (gate_act * (1.0 / (1.0 + jnp.exp(-gate_act))) * upward).astype(bf)
        for c in range(chunks):
            result = dot32(hidden, down_ref[:, span(c)]).astype(bf)
            for j in range(peers):
                served[k, c, j] = result[j * cap : (j + 1) * cap]
            for j in range(1, peers):
                third(k, c, j).start()
            back2[k, c, mine] = served[k, c, 0]

    def merge(k, local):
        at0, at1, info = slots(k)
        high = jnp.where(at0, info[:, 2:3], 0.0) + jnp.where(at1, info[:, 4:5], 0.0)
        low = jnp.where(at0, info[:, 3:4], 0.0) + jnp.where(at1, info[:, 5:6], 0.0)
        high = high.astype(bf)
        low = low.astype(bf)
        for c in range(chunks):
            for j in range(1, peers):
                third(k, c, j).wait_recv()
            got = back2[k, c].reshape(peers * cap, part)
            total = (dot32(high, got) + dot32(low, got)).astype(bf)
            if local:
                home[0, c] = total
            else:
                merged[k, c] = total
                fourth(k, c).start()

    scatter(0, True)
    scatter(recv_order[0], False)
    scatter(recv_order[1], False)
    serve(recv_order[0], True)
    serve(recv_order[1], False)
    merge(recv_order[0], False)
    scatter(recv_order[2], False)
    merge(recv_order[1], False)
    serve(recv_order[2], False)
    serve(0, False)
    merge(recv_order[2], False)
    merge(0, True)
    for c in range(chunks):
        total = stream_ref[:, span(c)] + dot_t(own, home[0, c])
        for k in send_order:
            fourth(k, c).wait_recv()
            total = total + dot_t(picks[(plane + k) % GROUPS], home[k, c])
        out_ref[:, span(c)] = total.astype(bf)
    for k in range(GROUPS):
        if k:
            note(k).wait_send()
        for c in range(chunks):
            if k:
                first(k, c).wait_send()
                fourth(k, c).wait_send()
            for j in range(1, peers):
                second(k, c, j).wait_send()
                third(k, c, j).wait_send()
    for m in range(1, n_y):
        across(0, m).wait_send()
    for k in range(1, GROUPS):

        @pl.when(plane + k < GROUPS)
        def _():
            up(k).wait_send()

        @pl.when(plane >= k)
        def _():
            for m in range(1, n_y):
                across(k, m).wait_send()


def per_device(
    residual,
    query,
    latent,
    rope_key,
    latent_gain,
    query_gain,
    key_gain,
    key_weight,
    value_weight,
    mix_gain,
    out_weight,
    ffn_gain,
    expert_choice,
    group_prob,
    expert_prob,
    gate_weight,
    up_weight,
    down_weight,
):
    n_sp = lax.axis_size("sp")
    n_dp = lax.axis_size("dp")
    n_y = n_sp // GROUPS
    _, tok, width = residual.shape
    rope = rope_key.shape[2]
    qk = query_gain.shape[0]
    nope = qk - rope
    heads = query.shape[2] // qk
    value_width = value_weight.shape[1] // heads
    lat = latent.shape[2]
    hidden = gate_weight.shape[2]
    experts = n_sp * n_dp
    peers = experts // GROUPS
    cap = tok * GROUPS // experts
    rows = peers * cap // expert_choice.shape[2]
    chunks = 4
    part = width // chunks
    bf = jnp.bfloat16
    f32 = jnp.float32
    phases = angles(0, n_sp * tok, rope).T
    operands = (
        residual[0],
        query[0],
        latent[0],
        rope_key[0].T,
        latent_gain[None],
        query_gain[None],
        key_gain[None],
        jnp.cos(phases),
        jnp.sin(phases),
        mix_gain[None],
        ffn_gain[None],
        expert_choice[0].T,
        group_prob,
        expert_prob[0].T,
        key_weight,
        value_weight,
        out_weight,
        gate_weight[0],
        up_weight[0],
        down_weight[0],
    )
    vmem = pl.BlockSpec(memory_space=pltpu.VMEM)
    hbm = pl.BlockSpec(memory_space=pl.ANY)
    dma = pltpu.SemaphoreType.DMA
    return pl.pallas_call(
        functools.partial(layer_kernel, n_sp, n_y, n_dp, heads, nope, rope, value_width, cap, rows),
        out_shape=jax.ShapeDtypeStruct((tok, width), bf),
        in_specs=[hbm] * len(operands),
        out_specs=vmem,
        scratch_shapes=[pltpu.VMEM(a.shape, a.dtype) for a in operands]
        + [
            pltpu.VMEM((8, 128), f32),
            pltpu.VMEM((n_sp, tok + rope // 2, lat), bf),
            pltpu.VMEM((heads, tok, qk), bf),
            pltpu.VMEM((n_y * tok, heads * value_width), bf),
            pltpu.VMEM((heads, tok, 128), f32),
            pltpu.VMEM((heads, tok, 2 * value_width), f32),
            pltpu.VMEM((tok, heads * value_width), bf),
            pltpu.VMEM((tok, width), f32),
            pltpu.VMEM((tok, width), bf),
            pltpu.VMEM((GROUPS, rows, tok), bf),
            pltpu.VMEM((GROUPS, rows, 128), bf),
            pltpu.VMEM((GROUPS, rows, 128), bf),
            pltpu.VMEM((GROUPS, chunks, rows, part), bf),
            pltpu.VMEM((GROUPS, chunks, rows, part), bf),
            pltpu.VMEM((GROUPS, chunks, peers, cap, part), bf),
            pltpu.VMEM((GROUPS, chunks, peers, cap, part), bf),
            pltpu.VMEM((GROUPS, chunks, peers, cap, part), bf),
            pltpu.VMEM((GROUPS, chunks, peers, cap, part), bf),
            pltpu.VMEM((GROUPS, chunks, rows, part), bf),
            pltpu.VMEM((GROUPS, chunks, rows, part), bf),
            dma((len(operands),)),
            dma((GROUPS,)),
            dma((GROUPS,)),
            dma((GROUPS, n_y)),
            dma((GROUPS, n_y)),
            dma((GROUPS,)),
            dma((GROUPS,)),
            dma((GROUPS, chunks)),
            dma((GROUPS, chunks)),
            dma((GROUPS, chunks, peers)),
            dma((GROUPS, chunks, peers)),
            dma((GROUPS, chunks, peers)),
            dma((GROUPS, chunks, peers)),
            dma((GROUPS, chunks)),
            dma((GROUPS, chunks)),
        ],
        compiler_params=pltpu.CompilerParams(
            collective_id=0, has_side_effects=True, vmem_limit_bytes=60 * 1024 * 1024
        ),
    )(*operands)[None]


def solution(mesh):
    return jax.shard_map(
        per_device,
        mesh=mesh,
        in_specs=(
            P("dp", "sp", None),
            P("dp", "sp", None),
            P("dp", "sp", None),
            P("dp", "sp", None),
            P(),
            P(),
            P(),
            P(),
            P(),
            P(),
            P(),
            P(),
            P("dp", "sp", None),
            P("dp", "sp"),
            P("dp", "sp", None),
            P(("sp", "dp"), None, None),
            P(("sp", "dp"), None, None),
            P(("sp", "dp"), None, None),
        ),
        out_specs=P("dp", "sp", None),
        check_vma=False,
    )
```

```python
import functools

import jax
import jax.numpy as jnp
import numpy as np
from jax import lax
from jax.experimental import pallas as pl
from jax.experimental.pallas import tpu as pltpu
from jax.sharding import PartitionSpec as P

GROUPS = 4
SPAN = 64


eps = 1e-06


def turns(length, rope_width):
    frequency = 10000.0 ** (-2.0 * np.arange(rope_width // 2) / rope_width)
    position = np.arange(length, dtype=np.float32)
    phases = (frequency.astype(np.float32)[:, None] * position[None, :]).astype(np.float64)
    return np.cos(phases).astype(np.float32), np.sin(phases).astype(np.float32)


def dot32(a, b):
    return jnp.dot(a, b, preferred_element_type=jnp.float32)


def dot_t(a, b):
    return lax.dot_general(a, b, (((0,), (0,)), ((), ())), preferred_element_type=jnp.float32)


def layer_kernel(
    n_sp,
    n_y,
    n_dp,
    heads,
    nope,
    rope,
    value_width,
    cap,
    rows,
    residual_hbm,
    query_hbm,
    latent_hbm,
    rope_hbm,
    latent_gain_hbm,
    query_gain_hbm,
    key_gain_hbm,
    cos_hbm,
    sin_hbm,
    mix_gain_hbm,
    ffn_gain_hbm,
    choice_hbm,
    group_prob_hbm,
    share_hbm,
    key_weight_hbm,
    value_weight_hbm,
    out_weight_hbm,
    gate_hbm,
    up_hbm,
    down_hbm,
    out_ref,
    residual_ref,
    query_ref,
    latent_ref,
    rope_ref,
    latent_gain_ref,
    query_gain_ref,
    key_gain_ref,
    cos_ref,
    sin_ref,
    mix_gain_ref,
    ffn_gain_ref,
    choice_ref,
    group_prob_ref,
    share_ref,
    key_weight_ref,
    value_weight_ref,
    out_weight_ref,
    gate_ref,
    up_ref,
    down_ref,
    gains,
    packed,
    queries,
    values,
    top,
    acc,
    heads_out,
    stream_ref,
    normed_ref,
    picks,
    notes_out,
    notes,
    out1,
    in1,
    out2,
    arrive,
    served,
    back2,
    merged,
    home,
    w_sem,
    sz,
    rz,
    sy,
    ry,
    s0,
    r0,
    s1,
    r1,
    s2,
    r2,
    s3,
    r3,
    s4,
    r4,
):
    bf = jnp.bfloat16
    f32 = jnp.float32
    tok = latent_ref.shape[0]
    qk = nope + rope
    half = rope // 2
    wide = 2 * value_width
    chunk = n_y * tok
    peers = n_y * n_dp
    chunks = in1.shape[1]
    part = in1.shape[3]
    me = lax.axis_index("sp")
    dp = lax.axis_index("dp")
    plane = me // n_y
    row = me % n_y
    mine = row * n_dp + dp

    def column(k):
        return {"sp": ((plane + k) % GROUPS) * n_y + row, "dp": dp}

    def peer(j):
        other = (mine + j) % peers
        return {"sp": plane * n_y + other // n_dp, "dp": other % n_dp}

    def at(index_plane, index_row):
        return {"sp": index_plane * n_y + index_row}

    barrier = pltpu.get_barrier_semaphore()
    for k in range(1, GROUPS):
        pl.semaphore_signal(barrier, inc=1, device_id=column(k), device_id_type=pl.DeviceIdType.MESH)
    for j in range(1, peers):
        pl.semaphore_signal(barrier, inc=1, device_id=peer(j), device_id_type=pl.DeviceIdType.MESH)

    pairs = (
        (latent_hbm, latent_ref),
        (latent_gain_hbm, latent_gain_ref),
        (rope_hbm, rope_ref),
        (choice_hbm, choice_ref),
        (group_prob_hbm, group_prob_ref),
        (share_hbm, share_ref),
        (query_gain_hbm, query_gain_ref),
        (key_gain_hbm, key_gain_ref),
        (cos_hbm, cos_ref),
        (sin_hbm, sin_ref),
        (query_hbm, query_ref),
        (key_weight_hbm, key_weight_ref),
        (value_weight_hbm, value_weight_ref),
        (residual_hbm, residual_ref),
        (mix_gain_hbm, mix_gain_ref),
        (ffn_gain_hbm, ffn_gain_ref),
        (out_weight_hbm, out_weight_ref),
        (gate_hbm, gate_ref),
        (up_hbm, up_ref),
        (down_hbm, down_ref),
    )
    copies = [
        (source, pltpu.make_async_copy(source, target, w_sem.at[i]))
        for i, (source, target) in enumerate(pairs)
    ]
    for _, copy in copies:
        copy.start()

    def ready(*sources):
        for source, copy in copies:
            if any(source is wanted for wanted in sources):
                copy.wait()

    def remote(src, dst, send, recv, target):
        return pltpu.make_async_remote_copy(
            src_ref=src,
            dst_ref=dst,
            send_sem=send,
            recv_sem=recv,
            device_id=target,
            device_id_type=pl.DeviceIdType.MESH,
        )

    def up(k):
        return remote(
            packed.at[me], packed.at[me], sz.at[k], rz.at[k], at((plane + k) % GROUPS, row)
        )

    def across(k, m):
        index = ((plane + GROUPS - k) % GROUPS) * n_y + row
        return remote(
            packed.at[index],
            packed.at[index],
            sy.at[k, m],
            ry.at[k, m],
            at(plane, (row + m) % n_y),
        )

    send_first = 1 + (plane + 1) // 2
    send_last = GROUPS - 1 - 2 * (plane // 2)
    send_order = (send_first, 6 - send_first - send_last, send_last)
    recv_first = 2 + (1 - plane // 2) * (1 - 2 * (plane % 2))
    recv_last = 1 + 2 * (plane % 2)
    recv_order = (recv_first, 6 - recv_first - recv_last, recv_last)

    def span(c):
        return slice(c * part, (c + 1) * part)

    def note(k):
        return remote(notes_out.at[k], notes.at[k], s0.at[k], r0.at[k], column(k))

    def first(k, c):
        return remote(out1.at[k, c], in1.at[k, c], s1.at[k, c], r1.at[k, c], column(k))

    def second(k, c, j):
        return remote(
            out2.at[k, c, (mine + j) % peers],
            arrive.at[k, c, j],
            s2.at[k, c, j],
            r2.at[k, c, j],
            peer(j),
        )

    def third(k, c, j):
        return remote(
            served.at[k, c, j],
            back2.at[k, c, mine],
            s3.at[k, c, j],
            r3.at[k, c, peers - j],
            peer(peers - j),
        )

    def fourth(k, c):
        return remote(merged.at[k, c], home.at[k, c], s4.at[k, c], r4.at[k, c], column(GROUPS - k))

    ready(latent_hbm, latent_gain_hbm, rope_hbm)
    raw = latent_ref[...].astype(f32)
    scale = lax.rsqrt(jnp.mean(raw * raw, axis=-1, keepdims=True) + eps)
    packed[me, :tok] = (raw * scale * latent_gain_ref[...]).astype(bf)
    packed[me, tok:, :tok] = rope_ref[:half]
    packed[me, tok:, tok : 2 * tok] = rope_ref[half:]
    pl.semaphore_wait(barrier, GROUPS - 1 + peers - 1)
    for k in send_order:

        @pl.when(plane + k < GROUPS)
        def _():
            up(k).start()

    for m in range(1, n_y):
        across(0, m).start()

    def positions(first, count):
        span = pl.ds(pl.multiple_of(first * tok, tok), count)
        return cos_ref[:, span], sin_ref[:, span]

    ready(query_gain_hbm, key_gain_hbm, cos_hbm, sin_hbm)
    gains[...] = jnp.zeros(gains.shape, f32)
    gains[0:1, :qk] = query_gain_ref[...]
    gains[1:2, :qk] = key_gain_ref[...]
    both = gains[...]
    lane = lax.broadcasted_iota(jnp.int32, (1, 128), 1)
    plain_gain = both[0:1] * jnp.where(lane < nope, both[1:2], 1.0)
    lower_gain = pltpu.roll(both, 128 - half, 1)[0:1]
    upper_gain = pltpu.roll(both, half, 1)[0:1]
    key_gains = jnp.broadcast_to(both[1:2], (128, 128)).T
    rope_low = key_gains[nope : nope + half, 0:1]
    rope_high = key_gains[nope + half : qk, 0:1]
    ready(query_hbm)
    cos, sin = positions(me, tok)
    pad = 128 - qk
    ones = jnp.ones((nope, tok), f32)
    none = jnp.zeros((half, tok), f32)
    empty = jnp.zeros((pad, tok), f32)
    zeros = jnp.zeros((nope, tok), f32)
    plain_table = jnp.concatenate([ones, cos, cos, empty], axis=0).T * plain_gain
    lower_table = jnp.concatenate([zeros, -sin, none, empty], axis=0).T * lower_gain
    upper_table = jnp.concatenate([zeros, none, sin, empty], axis=0).T * upper_gain
    lane = lax.broadcasted_iota(jnp.int32, (tok, 128), 1)
    for h in range(heads):
        base = h * qk // 128 * 128
        shift = h * qk - base
        if shift + qk <= 128:
            x = query_ref[:, base : base + 128].astype(f32)
            if shift:
                x = pltpu.roll(x, 128 - shift, 1)
        else:
            x = query_ref[:, base : base + 256].astype(f32)
            x = pltpu.roll(x, 256 - shift, 1)[:, :128]
        x = jnp.where(lane < qk, x, 0.0)
        scale = lax.rsqrt(jnp.sum(x * x, axis=-1, keepdims=True) / qk + eps)
        y = (
            x * plain_table
            + pltpu.roll(x, 128 - half, 1) * lower_table
            + pltpu.roll(x, half, 1) * upper_table
        )
        queries[h] = (y * scale)[:, :qk].astype(bf)


    ready(choice_hbm, group_prob_hbm, share_hbm)
    per_group = peers
    group = choice_ref[0:1] // per_group
    order = lax.broadcasted_iota(jnp.int32, (tok, tok), 0)
    sooner = order < lax.broadcasted_iota(jnp.int32, (tok, tok), 1)

    def tall(line):
        return jnp.broadcast_to(line.astype(f32), (tok, tok)).T

    def count(flags):
        return jnp.sum(jnp.where(sooner & flags, 1.0, 0.0), axis=0, keepdims=True)

    rank = count(tall(group) == group.astype(f32))
    line = group.astype(f32) * rows + rank
    for g in range(GROUPS):
        slot = g * rows + lax.broadcasted_iota(jnp.int32, (rows, tok), 0)
        picks[g] = jnp.where(slot.astype(f32) == line, 1.0, 0.0).astype(bf)
    talls = (tall(choice_ref[0:1]), tall(choice_ref[1:2]))
    facts = []
    for s in range(2):
        named = choice_ref[s : s + 1].astype(f32)
        earlier = count(talls[0] == named) + count(talls[1] == named)
        facts.append((named - group.astype(f32) * per_group) * cap + earlier)
    total = share_ref[0:1] + share_ref[1:2]
    for s in range(2):
        route = group_prob_ref[...] * share_ref[s : s + 1] / total
        high = route.astype(bf).astype(f32)
        facts.append(high)
        facts.append(route - high)
    facts.append(jnp.zeros((128 - len(facts), tok), f32))
    facts = jnp.concatenate(facts, axis=0).astype(bf)

    def describe(g):
        return lax.dot_general(
            picks[g], facts, (((1,), (1,)), ((), ())), preferred_element_type=f32
        ).astype(bf)

    notes[0] = describe(plane)
    for k in send_order:
        notes_out[k] = describe((plane + k) % GROUPS)
        note(k).start()

    def attend(k, first):
        base = (plane - k) * n_y
        blocks = [packed[base + r] for r in range(n_y)]
        latents = jnp.concatenate([block[:tok] for block in blocks], axis=0)
        values[...] = dot32(latents, value_weight_ref[...]).astype(bf)
        part = lax.dot_general(
            key_weight_ref[...], latents, (((0,), (1,)), ((), ())), preferred_element_type=f32
        ).astype(bf)
        low = jnp.concatenate([block[tok:, :tok] for block in blocks], axis=1).astype(f32)
        high = jnp.concatenate([block[tok:, tok : 2 * tok] for block in blocks], axis=1).astype(f32)
        shared = jnp.sum(low * low + high * high, axis=0, keepdims=True)
        cos, sin = positions(base, chunk)
        low = low * rope_low
        high = high * rope_high
        rope_keys = jnp.concatenate([low * cos - high * sin, high * cos + low * sin], axis=0).astype(bf)
        if first:
            q_pos = row * tok + lax.broadcasted_iota(jnp.int32, (tok, chunk), 0)
            k_pos = lax.broadcasted_iota(jnp.int32, (tok, chunk), 1)
            allowed = k_pos // SPAN <= q_pos // SPAN
        for h in range(heads):
            own = part[h * nope : (h + 1) * nope]
            square = own.astype(f32)
            square = jnp.sum(square * square, axis=0, keepdims=True)
            scale = lax.rsqrt((square + shared) / qk + eps) * (qk ** (-0.5) * 1.4426950408889634)
            scores = dot32(queries[h], jnp.concatenate([own, rope_keys], axis=0)) * scale
            if first:
                scores = jnp.where(allowed, scores, -1e30)
            peak = jnp.max(scores, axis=-1, keepdims=True)
            if not first:
                before = top[h][:, 0:1]
                peak = jnp.maximum(before, peak)
            raised = jnp.exp2(scores - peak).astype(bf)
            pair = values[:, h // 2 * wide : (h // 2 + 1) * wide]
            lanes = lax.broadcasted_iota(jnp.int32, pair.shape, 1)
            mine = (lanes < value_width) if h % 2 == 0 else (lanes >= value_width)
            summed = dot32(raised, jnp.where(mine, pair, jnp.ones_like(pair)))
            if first:
                acc[h] = summed
            else:
                acc[h] = acc[h] * jnp.exp2(before - peak) + summed
            top[h] = jnp.broadcast_to(peak, top.shape[1:])

    ready(key_weight_hbm, value_weight_hbm)

    def forward(k):
        up(k).wait_recv()
        for m in range(1, n_y):
            across(k, m).start()

    @pl.when(plane >= 1)
    def _():
        forward(1)

    for m in range(1, n_y):
        across(0, m).wait_recv()
    attend(0, True)

    def later(k, carry):
        @pl.when(plane >= k + 1)
        def _():
            forward(k + 1)

        for m in range(1, n_y):
            across(k, m).wait_recv()
        attend(k, False)
        return carry

    lax.fori_loop(1, plane + 1, later, 0)

    lanes = lax.broadcasted_iota(jnp.int32, (tok, wide), 1)
    square = None
    for p in range(heads // 2):
        even, odd = acc[2 * p], acc[2 * p + 1]
        total = jnp.where(lanes < value_width, odd, even)
        out = jnp.where(lanes < value_width, even, odd) / pltpu.roll(total, value_width, 1)
        out = out.astype(bf)
        heads_out[:, p * wide : (p + 1) * wide] = out
        out = out.astype(f32)
        term = jnp.sum(out * out, axis=-1, keepdims=True)
        square = term if square is None else square + term
    scale = lax.rsqrt(square / (heads * value_width) + eps)
    ready(mix_gain_hbm)
    mixed = (heads_out[...].astype(f32) * scale * mix_gain_ref[...]).astype(bf)
    ready(residual_hbm, ffn_gain_hbm, out_weight_hbm)
    stream = residual_ref[...].astype(f32) + dot32(mixed, out_weight_ref[...])
    stream_ref[...] = stream
    scale = lax.rsqrt(jnp.mean(stream * stream, axis=-1, keepdims=True) + eps)
    normed_ref[...] = (stream * scale * ffn_gain_ref[...]).astype(bf)
    everyone = jnp.concatenate(
        [picks[plane]] + [picks[(plane + k) % GROUPS] for k in send_order], axis=0
    )
    for c in range(chunks):
        packed_rows = dot32(everyone, normed_ref[:, span(c)]).astype(bf)
        in1[0, c] = packed_rows[:rows]
        for i, k in enumerate(send_order):
            out1[k, c] = packed_rows[(i + 1) * rows : (i + 2) * rows]
    for k in send_order:
        for c in range(chunks):
            first(k, c).start()

    def slots(k):
        info = notes[k].astype(jnp.float32)
        place = lax.broadcasted_iota(jnp.int32, (rows, peers * cap), 1).astype(jnp.float32)
        return place == info[:, 0:1], place == info[:, 1:2], info

    def scatter(k, local):
        if not local:
            note(k).wait_recv()
        at0, at1, _ = slots(k)
        choose = (at0.astype(jnp.float32) + at1.astype(jnp.float32)).astype(bf)
        for c in range(chunks):
            if not local:
                first(k, c).wait_recv()
            placed = dot_t(choose, in1[k, c]).astype(bf)
            for e in range(peers):
                out2[k, c, e] = placed[e * cap : (e + 1) * cap]
            for j in range(1, peers):
                second(k, c, j).start()
            arrive[k, c, 0] = out2[k, c, mine]

    def serve(k, load):
        gate_act = None
        for c in range(chunks):
            for j in range(1, peers):
                second(k, c, j).wait_recv()
            if load and c == 0:
                ready(gate_hbm, up_hbm, down_hbm)
            given = arrive[k, c].reshape(peers * cap, part)
            gate_part = dot32(given, gate_ref[span(c), :])
            up_part = dot32(given, up_ref[span(c), :])
            gate_act = gate_part if gate_act is None else gate_act + gate_part
            upward = up_part if c == 0 else upward + up_part
        hidden = (gate_act * (1.0 / (1.0 + jnp.exp(-gate_act))) * upward).astype(bf)
        for c in range(chunks):
            result = dot32(hidden, down_ref[:, span(c)]).astype(bf)
            for j in range(peers):
                served[k, c, j] = result[j * cap : (j + 1) * cap]
            for j in range(1, peers):
                third(k, c, j).start()
            back2[k, c, mine] = served[k, c, 0]

    def merge(k, local):
        at0, at1, info = slots(k)
        high = jnp.where(at0, info[:, 2:3], 0.0) + jnp.where(at1, info[:, 4:5], 0.0)
        low = jnp.where(at0, info[:, 3:4], 0.0) + jnp.where(at1, info[:, 5:6], 0.0)
        shares = jnp.concatenate([high, low], axis=0).astype(bf)
        for c in range(chunks):
            for j in range(1, peers):
                third(k, c, j).wait_recv()
            got = back2[k, c].reshape(peers * cap, part)
            total = dot32(shares, got)
            total = (total[:rows] + total[rows:]).astype(bf)
            if local:
                home[0, c] = total
            else:
                merged[k, c] = total
                fourth(k, c).start()

    scatter(0, True)
    scatter(recv_order[0], False)
    serve(0, True)
    scatter(recv_order[1], False)
    serve(recv_order[0], False)
    scatter(recv_order[2], False)
    merge(0, True)
    serve(recv_order[1], False)
    merge(recv_order[0], False)
    serve(recv_order[2], False)
    merge(recv_order[1], False)
    merge(recv_order[2], False)
    for c in range(chunks):
        for k in send_order:
            fourth(k, c).wait_recv()
        returned = jnp.concatenate([home[0, c]] + [home[k, c] for k in send_order], axis=0)
        total = stream_ref[:, span(c)] + dot_t(everyone, returned)
        out_ref[:, span(c)] = total.astype(bf)
    for k in range(GROUPS):
        if k:
            note(k).wait_send()
        for c in range(chunks):
            if k:
                first(k, c).wait_send()
                fourth(k, c).wait_send()
            for j in range(1, peers):
                second(k, c, j).wait_send()
                third(k, c, j).wait_send()
    for m in range(1, n_y):
        across(0, m).wait_send()
    for k in range(1, GROUPS):

        @pl.when(plane + k < GROUPS)
        def _():
            up(k).wait_send()

        @pl.when(plane >= k)
        def _():
            for m in range(1, n_y):
                across(k, m).wait_send()


def per_device(
    residual,
    query,
    latent,
    rope_key,
    latent_gain,
    query_gain,
    key_gain,
    key_weight,
    value_weight,
    mix_gain,
    out_weight,
    ffn_gain,
    expert_choice,
    group_prob,
    expert_prob,
    gate_weight,
    up_weight,
    down_weight,
):
    n_sp = lax.axis_size("sp")
    n_dp = lax.axis_size("dp")
    n_y = n_sp // GROUPS
    _, tok, width = residual.shape
    rope = rope_key.shape[2]
    qk = query_gain.shape[0]
    nope = qk - rope
    heads = query.shape[2] // qk
    value_width = value_weight.shape[1] // heads
    lat = latent.shape[2]
    hidden = gate_weight.shape[2]
    experts = n_sp * n_dp
    peers = experts // GROUPS
    cap = tok * GROUPS // experts
    rows = peers * cap // expert_choice.shape[2]
    chunks = 2
    part = width // chunks
    bf = jnp.bfloat16
    f32 = jnp.float32
    cos, sin = turns(n_sp * tok, rope)
    operands = (
        residual[0],
        query[0],
        latent[0],
        rope_key[0].T,
        latent_gain[None],
        query_gain[None],
        key_gain[None],
        jnp.asarray(cos),
        jnp.asarray(sin),
        mix_gain[None],
        ffn_gain[None],
        expert_choice[0].T,
        group_prob,
        expert_prob[0].T,
        key_weight,
        value_weight,
        out_weight,
        gate_weight[0],
        up_weight[0],
        down_weight[0],
    )
    vmem = pl.BlockSpec(memory_space=pltpu.VMEM)
    hbm = pl.BlockSpec(memory_space=pl.ANY)
    dma = pltpu.SemaphoreType.DMA
    return pl.pallas_call(
        functools.partial(layer_kernel, n_sp, n_y, n_dp, heads, nope, rope, value_width, cap, rows),
        out_shape=jax.ShapeDtypeStruct((tok, width), bf),
        in_specs=[hbm] * len(operands),
        out_specs=vmem,
        scratch_shapes=[pltpu.VMEM(a.shape, a.dtype) for a in operands]
        + [
            pltpu.VMEM((8, 128), f32),
            pltpu.VMEM((n_sp, tok + rope // 2, lat), bf),
            pltpu.VMEM((heads, tok, qk), bf),
            pltpu.VMEM((n_y * tok, heads * value_width), bf),
            pltpu.VMEM((heads, tok, 128), f32),
            pltpu.VMEM((heads, tok, 2 * value_width), f32),
            pltpu.VMEM((tok, heads * value_width), bf),
            pltpu.VMEM((tok, width), f32),
            pltpu.VMEM((tok, width), bf),
            pltpu.VMEM((GROUPS, rows, tok), bf),
            pltpu.VMEM((GROUPS, rows, 128), bf),
            pltpu.VMEM((GROUPS, rows, 128), bf),
            pltpu.VMEM((GROUPS, chunks, rows, part), bf),
            pltpu.VMEM((GROUPS, chunks, rows, part), bf),
            pltpu.VMEM((GROUPS, chunks, peers, cap, part), bf),
            pltpu.VMEM((GROUPS, chunks, peers, cap, part), bf),
            pltpu.VMEM((GROUPS, chunks, peers, cap, part), bf),
            pltpu.VMEM((GROUPS, chunks, peers, cap, part), bf),
            pltpu.VMEM((GROUPS, chunks, rows, part), bf),
            pltpu.VMEM((GROUPS, chunks, rows, part), bf),
            dma((len(operands),)),
            dma((GROUPS,)),
            dma((GROUPS,)),
            dma((GROUPS, n_y)),
            dma((GROUPS, n_y)),
            dma((GROUPS,)),
            dma((GROUPS,)),
            dma((GROUPS, chunks)),
            dma((GROUPS, chunks)),
            dma((GROUPS, chunks, peers)),
            dma((GROUPS, chunks, peers)),
            dma((GROUPS, chunks, peers)),
            dma((GROUPS, chunks, peers)),
            dma((GROUPS, chunks)),
            dma((GROUPS, chunks)),
        ],
        compiler_params=pltpu.CompilerParams(
            collective_id=0, has_side_effects=True, vmem_limit_bytes=60 * 1024 * 1024
        ),
    )(*operands)[None]


def solution(mesh):
    return jax.shard_map(
        per_device,
        mesh=mesh,
        in_specs=(
            P("dp", "sp", None),
            P("dp", "sp", None),
            P("dp", "sp", None),
            P("dp", "sp", None),
            P(),
            P(),
            P(),
            P(),
            P(),
            P(),
            P(),
            P(),
            P("dp", "sp", None),
            P("dp", "sp"),
            P("dp", "sp", None),
            P(("sp", "dp"), None, None),
            P(("sp", "dp"), None, None),
            P(("sp", "dp"), None, None),
        ),
        out_specs=P("dp", "sp", None),
        check_vma=False,
    )
```

```python
import functools

import jax
import jax.numpy as jnp
import numpy as np
from jax import lax
from jax.experimental import pallas as pl
from jax.experimental.pallas import tpu as pltpu
from jax.sharding import PartitionSpec as P

GROUPS = 4
SPAN = 64


eps = 1e-06


def turns(length, rope_width):
    frequency = 10000.0 ** (-2.0 * np.arange(rope_width // 2) / rope_width)
    position = np.arange(length, dtype=np.float32)
    phases = (frequency.astype(np.float32)[:, None] * position[None, :]).astype(np.float64)
    return np.cos(phases).astype(np.float32), np.sin(phases).astype(np.float32)


def dot32(a, b):
    return jnp.dot(a, b, preferred_element_type=jnp.float32)


def dot_t(a, b):
    return lax.dot_general(a, b, (((0,), (0,)), ((), ())), preferred_element_type=jnp.float32)


def layer_kernel(
    n_sp,
    n_y,
    n_dp,
    heads,
    nope,
    rope,
    value_width,
    cap,
    rows,
    residual_hbm,
    query_hbm,
    latent_hbm,
    rope_hbm,
    latent_gain_hbm,
    query_gain_hbm,
    key_gain_hbm,
    cos_hbm,
    sin_hbm,
    mix_gain_hbm,
    ffn_gain_hbm,
    choice_hbm,
    group_prob_hbm,
    share_hbm,
    key_weight_hbm,
    value_weight_hbm,
    out_weight_hbm,
    gate_hbm,
    up_hbm,
    down_hbm,
    out_ref,
    residual_ref,
    query_ref,
    latent_ref,
    rope_ref,
    latent_gain_ref,
    query_gain_ref,
    key_gain_ref,
    cos_ref,
    sin_ref,
    mix_gain_ref,
    ffn_gain_ref,
    choice_ref,
    group_prob_ref,
    share_ref,
    key_weight_ref,
    value_weight_ref,
    out_weight_ref,
    gate_ref,
    up_ref,
    down_ref,
    gains,
    packed,
    queries,
    values,
    top,
    acc,
    heads_out,
    stream_ref,
    normed_ref,
    picks,
    notes_out,
    notes,
    out1,
    in1,
    out2,
    arrive,
    served,
    back2,
    merged,
    home,
    w_sem,
    sz,
    rz,
    sy,
    ry,
    s0,
    r0,
    s1,
    r1,
    s2,
    r2,
    s3,
    r3,
    s4,
    r4,
):
    bf = jnp.bfloat16
    f32 = jnp.float32
    tok = latent_ref.shape[0]
    qk = nope + rope
    half = rope // 2
    wide = 2 * value_width
    chunk = n_y * tok
    peers = n_y * n_dp
    chunks = in1.shape[1]
    part = in1.shape[3]
    me = lax.axis_index("sp")
    dp = lax.axis_index("dp")
    plane = me // n_y
    row = me % n_y
    mine = row * n_dp + dp

    def column(k):
        return {"sp": ((plane + k) % GROUPS) * n_y + row, "dp": dp}

    def peer(j):
        other = (mine + j) % peers
        return {"sp": plane * n_y + other // n_dp, "dp": other % n_dp}

    def at(index_plane, index_row):
        return {"sp": index_plane * n_y + index_row}

    barrier = pltpu.get_barrier_semaphore()
    for k in range(1, GROUPS):
        pl.semaphore_signal(barrier, inc=1, device_id=column(k), device_id_type=pl.DeviceIdType.MESH)
    for j in range(1, peers):
        pl.semaphore_signal(barrier, inc=1, device_id=peer(j), device_id_type=pl.DeviceIdType.MESH)

    pairs = (
        (latent_hbm, latent_ref),
        (latent_gain_hbm, latent_gain_ref),
        (rope_hbm, rope_ref),
        (choice_hbm, choice_ref),
        (group_prob_hbm, group_prob_ref),
        (share_hbm, share_ref),
        (query_gain_hbm, query_gain_ref),
        (key_gain_hbm, key_gain_ref),
        (cos_hbm, cos_ref),
        (sin_hbm, sin_ref),
        (query_hbm, query_ref),
        (key_weight_hbm, key_weight_ref),
        (value_weight_hbm, value_weight_ref),
        (residual_hbm, residual_ref),
        (mix_gain_hbm, mix_gain_ref),
        (ffn_gain_hbm, ffn_gain_ref),
        (out_weight_hbm, out_weight_ref),
        (gate_hbm, gate_ref),
        (up_hbm, up_ref),
        (down_hbm, down_ref),
    )
    copies = [
        (source, pltpu.make_async_copy(source, target, w_sem.at[i]))
        for i, (source, target) in enumerate(pairs)
    ]
    for _, copy in copies:
        copy.start()

    def ready(*sources):
        for source, copy in copies:
            if any(source is wanted for wanted in sources):
                copy.wait()

    def remote(src, dst, send, recv, target):
        return pltpu.make_async_remote_copy(
            src_ref=src,
            dst_ref=dst,
            send_sem=send,
            recv_sem=recv,
            device_id=target,
            device_id_type=pl.DeviceIdType.MESH,
        )

    def up(k):
        return remote(
            packed.at[me], packed.at[me], sz.at[k], rz.at[k], at((plane + k) % GROUPS, row)
        )

    def across(k, m):
        index = ((plane + GROUPS - k) % GROUPS) * n_y + row
        return remote(
            packed.at[index],
            packed.at[index],
            sy.at[k, m],
            ry.at[k, m],
            at(plane, (row + m) % n_y),
        )

    send_first = 1 + (plane + 1) // 2
    send_last = GROUPS - 1 - 2 * (plane // 2)
    send_order = (send_first, 6 - send_first - send_last, send_last)
    recv_first = 2 + (1 - plane // 2) * (1 - 2 * (plane % 2))
    recv_last = 1 + 2 * (plane % 2)
    recv_order = (recv_first, 6 - recv_first - recv_last, recv_last)

    def span(c):
        return slice(c * part, (c + 1) * part)

    def note(k):
        return remote(notes_out.at[k], notes.at[k], s0.at[k], r0.at[k], column(k))

    def first(k, c):
        return remote(out1.at[k, c], in1.at[k, c], s1.at[k, c], r1.at[k, c], column(k))

    def second(k, c, j):
        return remote(
            out2.at[k, c, (mine + j) % peers],
            arrive.at[k, c, j],
            s2.at[k, c, j],
            r2.at[k, c, j],
            peer(j),
        )

    def third(k, c, j):
        return remote(
            served.at[k, c, j],
            back2.at[k, c, mine],
            s3.at[k, c, j],
            r3.at[k, c, peers - j],
            peer(peers - j),
        )

    def fourth(k, c):
        return remote(merged.at[k, c], home.at[k, c], s4.at[k, c], r4.at[k, c], column(GROUPS - k))

    ready(latent_hbm, latent_gain_hbm, rope_hbm)
    raw = latent_ref[...].astype(f32)
    scale = lax.rsqrt(jnp.mean(raw * raw, axis=-1, keepdims=True) + eps)
    packed[me, :tok] = (raw * scale * latent_gain_ref[...]).astype(bf)
    packed[me, tok:, :tok] = rope_ref[:half]
    packed[me, tok:, tok : 2 * tok] = rope_ref[half:]
    ready(choice_hbm, group_prob_hbm, share_hbm)
    per_group = peers
    group = choice_ref[0:1] // per_group
    order = lax.broadcasted_iota(jnp.int32, (tok, tok), 0)
    sooner = order < lax.broadcasted_iota(jnp.int32, (tok, tok), 1)

    def tall(line):
        return jnp.broadcast_to(line.astype(f32), (tok, tok)).T

    def count(flags):
        return jnp.sum(jnp.where(sooner & flags, 1.0, 0.0), axis=0, keepdims=True)

    rank = count(tall(group) == group.astype(f32))
    line = group.astype(f32) * rows + rank
    for g in range(GROUPS):
        slot = g * rows + lax.broadcasted_iota(jnp.int32, (rows, tok), 0)
        picks[g] = jnp.where(slot.astype(f32) == line, 1.0, 0.0).astype(bf)
    talls = (tall(choice_ref[0:1]), tall(choice_ref[1:2]))
    facts = []
    for s in range(2):
        named = choice_ref[s : s + 1].astype(f32)
        earlier = count(talls[0] == named) + count(talls[1] == named)
        facts.append((named - group.astype(f32) * per_group) * cap + earlier)
    total = share_ref[0:1] + share_ref[1:2]
    for s in range(2):
        route = group_prob_ref[...] * share_ref[s : s + 1] / total
        high = route.astype(bf).astype(f32)
        facts.append(high)
        facts.append(route - high)
    facts.append(jnp.zeros((128 - len(facts), tok), f32))
    facts = jnp.concatenate(facts, axis=0).astype(bf)

    def describe(g):
        return lax.dot_general(
            picks[g], facts, (((1,), (1,)), ((), ())), preferred_element_type=f32
        ).astype(bf)

    pl.semaphore_wait(barrier, GROUPS - 1 + peers - 1)
    for k in send_order:

        @pl.when(plane + k < GROUPS)
        def _():
            up(k).start()

    for m in range(1, n_y):
        across(0, m).start()

    def positions(first, count):
        span = pl.ds(pl.multiple_of(first * tok, tok), count)
        return cos_ref[:, span], sin_ref[:, span]

    ready(query_gain_hbm, key_gain_hbm, cos_hbm, sin_hbm)
    gains[...] = jnp.zeros(gains.shape, f32)
    gains[0:1, :qk] = query_gain_ref[...]
    gains[1:2, :qk] = key_gain_ref[...]
    both = gains[...]
    lane = lax.broadcasted_iota(jnp.int32, (1, 128), 1)
    plain_gain = both[0:1] * jnp.where(lane < nope, both[1:2], 1.0)
    lower_gain = pltpu.roll(both, 128 - half, 1)[0:1]
    upper_gain = pltpu.roll(both, half, 1)[0:1]
    key_gains = jnp.broadcast_to(both[1:2], (128, 128)).T
    rope_low = key_gains[nope : nope + half, 0:1]
    rope_high = key_gains[nope + half : qk, 0:1]
    ready(query_hbm)
    cos, sin = positions(me, tok)
    pad = 128 - qk
    ones = jnp.ones((nope, tok), f32)
    none = jnp.zeros((half, tok), f32)
    empty = jnp.zeros((pad, tok), f32)
    zeros = jnp.zeros((nope, tok), f32)
    plain_table = jnp.concatenate([ones, cos, cos, empty], axis=0).T * plain_gain
    lower_table = jnp.concatenate([zeros, -sin, none, empty], axis=0).T * lower_gain
    upper_table = jnp.concatenate([zeros, none, sin, empty], axis=0).T * upper_gain
    lane = lax.broadcasted_iota(jnp.int32, (tok, 128), 1)
    for h in range(heads):
        base = h * qk // 128 * 128
        shift = h * qk - base
        if shift + qk <= 128:
            x = query_ref[:, base : base + 128].astype(f32)
            if shift:
                x = pltpu.roll(x, 128 - shift, 1)
        else:
            x = query_ref[:, base : base + 256].astype(f32)
            x = pltpu.roll(x, 256 - shift, 1)[:, :128]
        x = jnp.where(lane < qk, x, 0.0)
        scale = lax.rsqrt(jnp.sum(x * x, axis=-1, keepdims=True) / qk + eps)
        y = (
            x * plain_table
            + pltpu.roll(x, 128 - half, 1) * lower_table
            + pltpu.roll(x, half, 1) * upper_table
        )
        queries[h] = (y * scale)[:, :qk].astype(bf)


    notes[0] = describe(plane)
    for k in send_order:
        notes_out[k] = describe((plane + k) % GROUPS)
        note(k).start()

    def attend(k, first):
        base = (plane - k) * n_y
        blocks = [packed[base + r] for r in range(n_y)]
        latents = jnp.concatenate([block[:tok] for block in blocks], axis=0)
        values[...] = dot32(latents, value_weight_ref[...]).astype(bf)
        part = lax.dot_general(
            key_weight_ref[...], latents, (((0,), (1,)), ((), ())), preferred_element_type=f32
        ).astype(bf)
        low = jnp.concatenate([block[tok:, :tok] for block in blocks], axis=1).astype(f32)
        high = jnp.concatenate([block[tok:, tok : 2 * tok] for block in blocks], axis=1).astype(f32)
        shared = jnp.sum(low * low + high * high, axis=0, keepdims=True)
        cos, sin = positions(base, chunk)
        low = low * rope_low
        high = high * rope_high
        rope_keys = jnp.concatenate([low * cos - high * sin, high * cos + low * sin], axis=0).astype(bf)
        if first:
            q_pos = row * tok + lax.broadcasted_iota(jnp.int32, (tok, chunk), 0)
            k_pos = lax.broadcasted_iota(jnp.int32, (tok, chunk), 1)
            allowed = k_pos // SPAN <= q_pos // SPAN
        for h in range(heads):
            own = part[h * nope : (h + 1) * nope]
            square = own.astype(f32)
            square = jnp.sum(square * square, axis=0, keepdims=True)
            scale = lax.rsqrt((square + shared) / qk + eps) * (qk ** (-0.5) * 1.4426950408889634)
            scores = dot32(queries[h], jnp.concatenate([own, rope_keys], axis=0)) * scale
            if first:
                scores = jnp.where(allowed, scores, -1e30)
            peak = jnp.max(scores, axis=-1, keepdims=True)
            if not first:
                before = top[h][:, 0:1]
                peak = jnp.maximum(before, peak)
            raised = jnp.exp2(scores - peak).astype(bf)
            pair = values[:, h // 2 * wide : (h // 2 + 1) * wide]
            lanes = lax.broadcasted_iota(jnp.int32, pair.shape, 1)
            mine = (lanes < value_width) if h % 2 == 0 else (lanes >= value_width)
            summed = dot32(raised, jnp.where(mine, pair, jnp.ones_like(pair)))
            if first:
                acc[h] = summed
            else:
                acc[h] = acc[h] * jnp.exp2(before - peak) + summed
            top[h] = jnp.broadcast_to(peak, top.shape[1:])

    ready(key_weight_hbm, value_weight_hbm)

    def forward(k):
        up(k).wait_recv()
        for m in range(1, n_y):
            across(k, m).start()

    @pl.when(plane >= 1)
    def _():
        forward(1)

    for m in range(1, n_y):
        across(0, m).wait_recv()
    attend(0, True)

    def later(k, carry):
        @pl.when(plane >= k + 1)
        def _():
            forward(k + 1)

        for m in range(1, n_y):
            across(k, m).wait_recv()
        attend(k, False)
        return carry

    lax.fori_loop(1, plane + 1, later, 0)

    lanes = lax.broadcasted_iota(jnp.int32, (tok, wide), 1)
    square = None
    for p in range(heads // 2):
        even, odd = acc[2 * p], acc[2 * p + 1]
        total = jnp.where(lanes < value_width, odd, even)
        out = jnp.where(lanes < value_width, even, odd) / pltpu.roll(total, value_width, 1)
        out = out.astype(bf)
        heads_out[:, p * wide : (p + 1) * wide] = out
        out = out.astype(f32)
        term = jnp.sum(out * out, axis=-1, keepdims=True)
        square = term if square is None else square + term
    scale = lax.rsqrt(square / (heads * value_width) + eps)
    ready(mix_gain_hbm)
    mixed = (heads_out[...].astype(f32) * scale * mix_gain_ref[...]).astype(bf)
    ready(residual_hbm, ffn_gain_hbm, out_weight_hbm)
    stream = residual_ref[...].astype(f32) + dot32(mixed, out_weight_ref[...])
    stream_ref[...] = stream
    scale = lax.rsqrt(jnp.mean(stream * stream, axis=-1, keepdims=True) + eps)
    normed_ref[...] = (stream * scale * ffn_gain_ref[...]).astype(bf)
    everyone = jnp.concatenate(
        [picks[plane]] + [picks[(plane + k) % GROUPS] for k in send_order], axis=0
    )
    for c in range(chunks):
        packed_rows = dot32(everyone, normed_ref[:, span(c)]).astype(bf)
        in1[0, c] = packed_rows[:rows]
        for i, k in enumerate(send_order):
            out1[k, c] = packed_rows[(i + 1) * rows : (i + 2) * rows]
    for k in send_order:
        for c in range(chunks):
            first(k, c).start()

    def slots(k):
        info = notes[k].astype(jnp.float32)
        place = lax.broadcasted_iota(jnp.int32, (rows, peers * cap), 1).astype(jnp.float32)
        return place == info[:, 0:1], place == info[:, 1:2], info

    def scatter(k, local):
        if not local:
            note(k).wait_recv()
        at0, at1, _ = slots(k)
        choose = (at0.astype(jnp.float32) + at1.astype(jnp.float32)).astype(bf)
        for c in range(chunks):
            if not local:
                first(k, c).wait_recv()
            placed = dot_t(choose, in1[k, c]).astype(bf)
            for e in range(peers):
                out2[k, c, e] = placed[e * cap : (e + 1) * cap]
            for j in range(1, peers):
                second(k, c, j).start()
            arrive[k, c, 0] = out2[k, c, mine]

    def serve(k, load):
        gate_act = None
        for c in range(chunks):
            for j in range(1, peers):
                second(k, c, j).wait_recv()
            if load and c == 0:
                ready(gate_hbm, up_hbm, down_hbm)
            given = arrive[k, c].reshape(peers * cap, part)
            gate_part = dot32(given, gate_ref[span(c), :])
            up_part = dot32(given, up_ref[span(c), :])
            gate_act = gate_part if gate_act is None else gate_act + gate_part
            upward = up_part if c == 0 else upward + up_part
        hidden = (gate_act * (1.0 / (1.0 + jnp.exp(-gate_act))) * upward).astype(bf)
        for c in range(chunks):
            result = dot32(hidden, down_ref[:, span(c)]).astype(bf)
            for j in range(peers):
                served[k, c, j] = result[j * cap : (j + 1) * cap]
            for j in range(1, peers):
                third(k, c, j).start()
            back2[k, c, mine] = served[k, c, 0]

    def merge(k, local):
        at0, at1, info = slots(k)
        high = jnp.where(at0, info[:, 2:3], 0.0) + jnp.where(at1, info[:, 4:5], 0.0)
        low = jnp.where(at0, info[:, 3:4], 0.0) + jnp.where(at1, info[:, 5:6], 0.0)
        shares = jnp.concatenate([high, low], axis=0).astype(bf)
        for c in range(chunks):
            for j in range(1, peers):
                third(k, c, j).wait_recv()
            got = back2[k, c].reshape(peers * cap, part)
            total = dot32(shares, got)
            total = (total[:rows] + total[rows:]).astype(bf)
            if local:
                home[0, c] = total
            else:
                merged[k, c] = total
                fourth(k, c).start()

    scatter(0, True)
    scatter(recv_order[0], False)
    serve(0, True)
    scatter(recv_order[1], False)
    serve(recv_order[0], False)
    scatter(recv_order[2], False)
    serve(recv_order[1], False)
    merge(recv_order[0], False)
    merge(0, True)
    serve(recv_order[2], False)
    merge(recv_order[1], False)
    merge(recv_order[2], False)
    for c in range(chunks):
        for k in send_order:
            fourth(k, c).wait_recv()
        returned = jnp.concatenate([home[0, c]] + [home[k, c] for k in send_order], axis=0)
        total = stream_ref[:, span(c)] + dot_t(everyone, returned)
        out_ref[:, span(c)] = total.astype(bf)
    for k in range(GROUPS):
        if k:
            note(k).wait_send()
        for c in range(chunks):
            if k:
                first(k, c).wait_send()
                fourth(k, c).wait_send()
            for j in range(1, peers):
                second(k, c, j).wait_send()
                third(k, c, j).wait_send()
    for m in range(1, n_y):
        across(0, m).wait_send()
    for k in range(1, GROUPS):

        @pl.when(plane + k < GROUPS)
        def _():
            up(k).wait_send()

        @pl.when(plane >= k)
        def _():
            for m in range(1, n_y):
                across(k, m).wait_send()


def per_device(
    residual,
    query,
    latent,
    rope_key,
    latent_gain,
    query_gain,
    key_gain,
    key_weight,
    value_weight,
    mix_gain,
    out_weight,
    ffn_gain,
    expert_choice,
    group_prob,
    expert_prob,
    gate_weight,
    up_weight,
    down_weight,
):
    n_sp = lax.axis_size("sp")
    n_dp = lax.axis_size("dp")
    n_y = n_sp // GROUPS
    _, tok, width = residual.shape
    rope = rope_key.shape[2]
    qk = query_gain.shape[0]
    nope = qk - rope
    heads = query.shape[2] // qk
    value_width = value_weight.shape[1] // heads
    lat = latent.shape[2]
    hidden = gate_weight.shape[2]
    experts = n_sp * n_dp
    peers = experts // GROUPS
    cap = tok * GROUPS // experts
    rows = peers * cap // expert_choice.shape[2]
    chunks = 2
    part = width // chunks
    bf = jnp.bfloat16
    f32 = jnp.float32
    cos, sin = turns(n_sp * tok, rope)
    operands = (
        residual[0],
        query[0],
        latent[0],
        rope_key[0].T,
        latent_gain[None],
        query_gain[None],
        key_gain[None],
        jnp.asarray(cos),
        jnp.asarray(sin),
        mix_gain[None],
        ffn_gain[None],
        expert_choice[0].T,
        group_prob,
        expert_prob[0].T,
        key_weight,
        value_weight,
        out_weight,
        gate_weight[0],
        up_weight[0],
        down_weight[0],
    )
    vmem = pl.BlockSpec(memory_space=pltpu.VMEM)
    hbm = pl.BlockSpec(memory_space=pl.ANY)
    dma = pltpu.SemaphoreType.DMA
    return pl.pallas_call(
        functools.partial(layer_kernel, n_sp, n_y, n_dp, heads, nope, rope, value_width, cap, rows),
        out_shape=jax.ShapeDtypeStruct((tok, width), bf),
        in_specs=[hbm] * len(operands),
        out_specs=vmem,
        scratch_shapes=[pltpu.VMEM(a.shape, a.dtype) for a in operands]
        + [
            pltpu.VMEM((8, 128), f32),
            pltpu.VMEM((n_sp, tok + rope // 2, lat), bf),
            pltpu.VMEM((heads, tok, qk), bf),
            pltpu.VMEM((n_y * tok, heads * value_width), bf),
            pltpu.VMEM((heads, tok, 128), f32),
            pltpu.VMEM((heads, tok, 2 * value_width), f32),
            pltpu.VMEM((tok, heads * value_width), bf),
            pltpu.VMEM((tok, width), f32),
            pltpu.VMEM((tok, width), bf),
            pltpu.VMEM((GROUPS, rows, tok), bf),
            pltpu.VMEM((GROUPS, rows, 128), bf),
            pltpu.VMEM((GROUPS, rows, 128), bf),
            pltpu.VMEM((GROUPS, chunks, rows, part), bf),
            pltpu.VMEM((GROUPS, chunks, rows, part), bf),
            pltpu.VMEM((GROUPS, chunks, peers, cap, part), bf),
            pltpu.VMEM((GROUPS, chunks, peers, cap, part), bf),
            pltpu.VMEM((GROUPS, chunks, peers, cap, part), bf),
            pltpu.VMEM((GROUPS, chunks, peers, cap, part), bf),
            pltpu.VMEM((GROUPS, chunks, rows, part), bf),
            pltpu.VMEM((GROUPS, chunks, rows, part), bf),
            dma((len(operands),)),
            dma((GROUPS,)),
            dma((GROUPS,)),
            dma((GROUPS, n_y)),
            dma((GROUPS, n_y)),
            dma((GROUPS,)),
            dma((GROUPS,)),
            dma((GROUPS, chunks)),
            dma((GROUPS, chunks)),
            dma((GROUPS, chunks, peers)),
            dma((GROUPS, chunks, peers)),
            dma((GROUPS, chunks, peers)),
            dma((GROUPS, chunks, peers)),
            dma((GROUPS, chunks)),
            dma((GROUPS, chunks)),
        ],
        compiler_params=pltpu.CompilerParams(
            collective_id=0, has_side_effects=True, vmem_limit_bytes=60 * 1024 * 1024
        ),
    )(*operands)[None]


def solution(mesh):
    return jax.shard_map(
        per_device,
        mesh=mesh,
        in_specs=(
            P("dp", "sp", None),
            P("dp", "sp", None),
            P("dp", "sp", None),
            P("dp", "sp", None),
            P(),
            P(),
            P(),
            P(),
            P(),
            P(),
            P(),
            P(),
            P("dp", "sp", None),
            P("dp", "sp"),
            P("dp", "sp", None),
            P(("sp", "dp"), None, None),
            P(("sp", "dp"), None, None),
            P(("sp", "dp"), None, None),
        ),
        out_specs=P("dp", "sp", None),
        check_vma=False,
    )
```
